256 devices in a mesh: grp: 2 (over y), ep: 32 (over z, core), tp: 4 (over x).
Axes of the slice: x: 4, y: 2, z: 16, core: 2. Of those that a mesh axis runs over, the one named last changes fastest.
The devices are a block of a 4x16x16 slice.
Arguments:
- queries: bfloat16 [16384, 1024], P(('grp', 'ep'), 'tp'), parts along dimension 0, may hold values from -6 to 6
- head_key_rows: bfloat16 [16384, 1024], P(('grp', 'ep'), 'tp'), parts along dimension 0, may hold values from -6 to 6
- head_value_rows: bfloat16 [16384, 2048], P(('grp', 'ep'), 'tp'), parts along dimension 0, may hold values from -6 to 6
- output_gate_logits: bfloat16 [16384, 2048], P(('grp', 'ep'), 'tp'), parts along dimension 0, may hold values from -6 to 6
- log_input_gate: float32 [4, 16384], P('tp', ('grp', 'ep')), parts along dimension 1, may hold values from -5 to 103
- forget_gate_logits: float32 [4, 16384], P('tp', ('grp', 'ep')), parts along dimension 1, may hold values from 1 to 20
- extra_log_forget: float32 [4, 16384], P('tp', ('grp', 'ep')), parts along dimension 1, may hold values from -1 to 0, as said below
- head_norm_gain: float32 [2048], P('tp'), may hold values from 0.1 to 1.9
- memory_output_matrix: bfloat16 [2048, 2048], P('tp'), may hold values from -0.125 to 0.125
- expert_input_tokens: bfloat16 [16384, 2048], P(('grp', 'ep', 'tp')), parts along dimension 0, may hold values from -6 to 6
- expert_norm_gain: float32 [2048], replicated, may hold values from 0.1 to 1.9
- routes: int32 [16384, 2], P(('grp', 'ep', 'tp')), parts along dimension 0, may hold values from 0 to 127, all different within a row; in each aligned block of 64 rows (0 to 63, 64 to 127, ...) at most 2 rows name the same one
- routed_expert_weight: float32 [16384, 2], P(('grp', 'ep', 'tp')), parts along dimension 0, may hold values from 0.1 to 1
- expert_gate_matrix: bfloat16 [128, 2048, 512], P(('ep', 'tp')), may hold values from -0.125 to 0.125
- expert_up_matrix: bfloat16 [128, 2048, 512], P(('ep', 'tp')), may hold values from -0.125 to 0.125
- expert_down_matrix: bfloat16 [128, 512, 2048], P(('ep', 'tp')), may hold values from -0.25 to 0.25
Outputs:
- mixer_out: bfloat16 [16384, 2048], P(('grp', 'ep', 'tp')), parts along dimension 0
- expert_out: bfloat16 [16384, 2048], P(('grp', 'ep', 'tp')), parts along dimension 0
The draws below stay inside these ranges and needn't reach their ends.
There are 2 independent parts, one for each index of `grp`. The reference program is written for one: setup_inputs(seed, part) draws one part's arguments, and reference() takes and returns one part's arrays. A program takes and returns all parts, laid end to end along the dimension named above; an argument that names none is the same for every part. Nothing has to cross between parts.
Inputs may be any that keep to these rules, and one draw needn't show every extreme that they name: `routes`: each row names 2 different experts. In the rows of one device (aligned blocks of 64 rows) no expert is named more than 2 times, and in some blocks one expert is named exactly 2 times. `extra_log_forget`: mostly zero.
All inputs are finite; a program needn't handle non-finite values.
Results may differ from the reference program's by a relative error of at most 0.009.
Values may be sent and summed in bfloat16 or wider, within the bound.
A program may use at most 128 MiB of HBM per device.

```python
import math
import jax
import jax.numpy as jnp
import numpy as np
from jax import lax

D = 2048
HEADS = 4
DQK = 256
DV = 512
FE = 512
TOP = 2
TOKB_DEV = 64
EXPERTS = 128
SPAN = 256
SEQ_A = 8192
TOKENS_B = 8192
CAP = 2
N_EP = 32
N_TP = 4


def draw_log_input_gate(key, part):
    drawn = jax.random.uniform(key, (HEADS, SEQ_A), jnp.float32, -5.0, 3.0)
    return drawn


def draw_forget_gate_logits(key, part):
    order_key = jax.random.fold_in(key, 11)
    shift_key = jax.random.fold_in(key, 12)
    noise_key = jax.random.fold_in(key, 13)
    head_order = jax.random.permutation(order_key, HEADS)
    head_rank = jnp.argsort(head_order)
    fast_count = HEADS // 2
    slow_base = math.log(SEQ_A) + 1.0
    base_level = jnp.where(head_rank < fast_count, 3.5, slow_base).astype(jnp.float32)
    block_shift = jax.random.uniform(shift_key, (HEADS, SEQ_A // SPAN), jnp.float32, -0.8, 0.8)
    block_shift = jnp.repeat(block_shift, SPAN, axis=1)
    noise = jax.random.uniform(noise_key, (HEADS, SEQ_A), jnp.float32, -1.0, 1.0)
    return base_level[:, None] + block_shift + noise


def draw_extra_log_forget(key, part):
    spot_key = jax.random.fold_in(key, 21)
    drop_key = jax.random.fold_in(key, 22)
    spots = jax.random.randint(spot_key, (HEADS, 3), 0, SEQ_A)
    drops = jax.random.uniform(drop_key, (HEADS, 3), jnp.float32, -0.5, -0.22)
    places = jnp.arange(SEQ_A)[None, None, :] == spots[:, :, None]
    return jnp.sum(jnp.where(places, drops[:, :, None], 0.0), axis=1).astype(jnp.float32)


def block_levels(stream_key, extent, split, least, top_value):
    loudness = 1.0
    for axis_at, parts in split:
        draws = jax.random.uniform(jax.random.fold_in(jax.random.fold_in(stream_key, 6), axis_at), (parts,), jnp.float32, least / len(split), top_value / len(split))
        loudness = loudness * jnp.repeat(jnp.exp(draws), extent[axis_at] // parts).reshape((-1,) + (1,) * (len(extent) - 1 - axis_at))
    return loudness


def routed_block(key, own, number, rows, number_of, top, most, lean):
    order = jax.random.permutation(key, number_of)
    packed, usual = shares(number_of, rows * top, most, lean, True), shares(number_of, rows * top, most, lean, False)
    places = jnp.arange(number_of)

    def named(lengths, offset_by):
        used = int((lengths > 0).sum())
        fixed = max(1, used // 4)
        passed = fixed + (places - fixed + offset_by * (used - fixed)) % max(1, number_of - fixed)
        return jnp.zeros((number_of,), jnp.int32).at[order[jnp.where(places < fixed, places, passed)]].set(jnp.asarray(lengths, jnp.int32))

    lengths = jnp.where(number % 4 == 0, named(packed, number // 4), named(usual, number - number // 4 - 1))
    mixed = jax.random.permutation(jax.random.fold_in(own, 3), number_of)
    donor, receiver = mixed[0:number_of // 2 * 2:2], mixed[1:number_of // 2 * 2:2]
    slack = jnp.minimum(lengths[donor] - 1, most - lengths[receiver]) // 2
    slack = jnp.where((donor == order[0]) | (receiver == order[0]) | (lengths[receiver] == 0), 0, jnp.maximum(slack, 0))
    passed = jax.random.randint(jax.random.fold_in(own, 4), (number_of // 2,), 0, 1 << 20) % (slack + 1)
    lengths = lengths.at[donor].add(-passed).at[receiver].add(passed)
    items = jnp.searchsorted(jnp.cumsum(lengths), jnp.arange(rows * top), side="right").astype(jnp.int32)
    table = items.reshape(top, rows).T
    table = table[jax.random.permutation(jax.random.fold_in(own, 1), rows)]
    offset_by = jax.random.randint(jax.random.fold_in(own, 2), (rows, 1), 0, top)
    return jnp.take_along_axis(table, (jnp.arange(top)[None, :] + offset_by) % top, axis=1)


def shares(number_of, total, most, slope, full):
    loads = [(1 << 20) // math.isqrt(standing ** slope) + 1 for standing in range(1, number_of + 1)]
    largest = most if full else min(most, max(-(-total // number_of), total * loads[0] // sum(loads)))
    least = 1 if total - largest >= number_of - 1 else 0
    holding, rest = [largest] + [least] * (number_of - 1), total - largest - least * (number_of - 1)
    while rest > 0:
        movable = [i for i in range(1, number_of) if holding[i] < largest] or [i for i in range(1, number_of) if holding[i] < most]
        mass, remaining = sum([loads[i] for i in movable]), rest
        for i in movable:
            more = min(most - holding[i], max(1, remaining * loads[i] // mass), rest)
            holding[i] = holding[i] + more
            rest = rest - more
    return np.array(holding)


def gaussian(stream_key, dims, scale, limit, shards=(), kind=jnp.bfloat16):
    loudness = block_levels(stream_key, dims, shards, -0.22, 0.18) if shards else 1.0
    result = jax.random.normal(stream_key, dims, jnp.float32) * scale * loudness
    return jnp.minimum(jnp.maximum(result, -limit), limit).astype(kind)


def setup_inputs(seed: int = 0, part: int = 0) -> dict:
    splits = jax.random.split(jax.random.key(seed), 17)
    part_keys = jax.random.split(jax.random.fold_in(splits[16], part), 17)
    queries = gaussian(part_keys[0], (SEQ_A, HEADS * DQK), 1.0, 6.0, ((0, 32), (1, 4)))
    head_key_rows = gaussian(part_keys[1], (SEQ_A, HEADS * DQK), 1.0, 6.0, ((0, 32), (1, 4)))
    head_value_rows = gaussian(part_keys[2], (SEQ_A, HEADS * DV), 1.0, 6.0, ((0, 32), (1, 4)))
    output_gate_logits = gaussian(part_keys[3], (SEQ_A, HEADS * DV), 1.0, 6.0, ((0, 32), (1, 4)))
    log_input_gate = draw_log_input_gate(jax.random.fold_in(jax.random.fold_in(splits[16], part), 71), part)
    forget_gate_logits = draw_forget_gate_logits(jax.random.fold_in(jax.random.fold_in(splits[16], part), 71), part)
    extra_log_forget = draw_extra_log_forget(jax.random.fold_in(jax.random.fold_in(splits[16], part), 71), part)
    head_norm_gain = jnp.clip(1.0 + 0.18 * jax.random.normal(splits[7], (HEADS * DV,), jnp.float32), 0.1, 1.9)
    memory_output_matrix = gaussian(splits[8], (HEADS * DV, D), (HEADS * DV) ** -0.5, 0.125, ((0, 4),))
    expert_input_tokens = gaussian(part_keys[9], (TOKENS_B, D), 1.0, 6.0, ((0, 128),))
    expert_norm_gain = jnp.clip(1.0 + 0.18 * jax.random.normal(splits[10], (D,), jnp.float32), 0.1, 1.9)
    routes_keys = jax.random.split(jax.random.fold_in(part_keys[11], 1), TOKENS_B // TOKB_DEV)
    routes_turns = jax.random.permutation(jax.random.fold_in(part_keys[11], 3), TOKENS_B // TOKB_DEV)
    routes = jax.vmap(lambda own, number: routed_block(jax.random.fold_in(part_keys[11], 2), own, number, TOKB_DEV, EXPERTS, TOP, CAP, 1))(routes_keys, routes_turns).reshape((TOKENS_B, TOP))
    routed_expert_weight = jnp.clip(0.1 + 0.9 * jax.random.uniform(part_keys[12], (TOKENS_B, TOP), jnp.float32) ** block_levels(part_keys[12], (TOKENS_B, TOP), ((0, 128),), -0.2, 0.2), 0.1, 1.0)
    expert_gate_matrix = gaussian(splits[13], (EXPERTS, D, FE), D ** -0.5, 0.125, ((0, 128),))
    expert_up_matrix = gaussian(splits[14], (EXPERTS, D, FE), D ** -0.5, 0.125, ((0, 128),))
    expert_down_matrix = gaussian(splits[15], (EXPERTS, FE, D), FE ** -0.5, 0.25, ((0, 128),))
    return {"queries": queries, "head_key_rows": head_key_rows, "head_value_rows": head_value_rows, "output_gate_logits": output_gate_logits, "log_input_gate": log_input_gate, "forget_gate_logits": forget_gate_logits, "extra_log_forget": extra_log_forget, "head_norm_gain": head_norm_gain, "memory_output_matrix": memory_output_matrix, "expert_input_tokens": expert_input_tokens, "expert_norm_gain": expert_norm_gain, "routes": routes, "routed_expert_weight": routed_expert_weight, "expert_gate_matrix": expert_gate_matrix, "expert_up_matrix": expert_up_matrix, "expert_down_matrix": expert_down_matrix}


lowest_log = -1e+30
norm_eps = 1e-06
layer_eps = 1e-05

def join_states(earlier, later):
    early_memory, early_top, early_total = earlier
    late_memory, late_top, late_total = later
    joined_top = jnp.maximum(late_total + early_top, late_top)
    joined_memory = jnp.exp(late_total + early_top - joined_top) * early_memory + jnp.exp(late_top - joined_top) * late_memory
    return (joined_memory, joined_top, early_total + late_total)

def block_summary(keys_f32, values_f32, log_weight):
    top_weight = jnp.max(log_weight)
    weighted = keys_f32 * jnp.exp(log_weight - top_weight)[:, None]
    memory = jnp.einsum('sd,se->de', weighted, values_f32, precision=lax.Precision.HIGHEST)
    return (memory, top_weight)

def block_output(queries, head_key_rows, head_value_rows, output_gate_logits, in_gate, through, before, span_total, prior_memory, prior_top, later_memory, later_top, head_norm_gain):
    score_scale = queries.shape[1] ** (-0.5)
    from_prior = through + prior_top
    from_later = span_total - before + later_top
    fw_log = through[:, None] - through[None, :] + in_gate[None, :]
    bw_log = before[None, :] - before[:, None] + in_gate[None, :]
    positions = jnp.arange(queries.shape[0])
    lower_mask = positions[:, None] >= positions[None, :]
    upper_mask = positions[:, None] <= positions[None, :]
    inner_top = jnp.maximum(lax.optimization_barrier(jnp.max(jnp.where(lower_mask, fw_log, -jnp.inf), axis=1)), lax.optimization_barrier(jnp.max(jnp.where(upper_mask, bw_log, -jnp.inf), axis=1)))
    row_top = jnp.maximum(inner_top, jnp.maximum(from_prior, from_later))
    weights = jnp.where(lower_mask, jnp.exp(fw_log - row_top[:, None]), 0.0) + jnp.where(upper_mask, jnp.exp(bw_log - row_top[:, None]), 0.0)
    scores = jnp.einsum('td,sd->ts', queries, head_key_rows, preferred_element_type=jnp.float32) * score_scale
    near_weights = (scores * weights).astype(jnp.bfloat16)
    queries_f32 = queries.astype(jnp.float32)
    carried = jnp.exp(from_prior - row_top)[:, None] * jnp.dot(queries_f32, prior_memory, precision=lax.Precision.HIGHEST)
    carried = carried + jnp.exp(from_later - row_top)[:, None] * jnp.dot(queries_f32, later_memory, precision=lax.Precision.HIGHEST)
    head_rows = jnp.dot(near_weights, head_value_rows, preferred_element_type=jnp.float32) + carried * score_scale
    normed = head_rows * lax.rsqrt(lax.optimization_barrier(jnp.mean(head_rows * head_rows, axis=1, keepdims=True)) + norm_eps) * head_norm_gain
    return (jax.nn.sigmoid(output_gate_logits.astype(jnp.float32)) * normed).astype(jnp.bfloat16)

def mixer_head(queries, head_key_rows, head_value_rows, output_gate_logits, in_gate, forget_log_value, head_norm_gain):
    blocks = queries.shape[0] // SPAN

    def split_rows(stacked):
        return stacked.reshape((blocks, SPAN) + stacked.shape[1:])
    query_blocks = split_rows(queries)
    key_blocks = split_rows(head_key_rows)
    value_blocks = split_rows(head_value_rows)
    gate_blocks = split_rows(output_gate_logits)
    input_blocks = split_rows(in_gate)
    forget_blocks = split_rows(forget_log_value)
    through = jnp.cumsum(forget_blocks, axis=1)
    before = through - forget_blocks
    span_total = through[:, -1]
    keys_f32 = key_blocks.astype(jnp.float32)
    values_f32 = value_blocks.astype(jnp.float32)
    fw_memory, fw_top = jax.vmap(block_summary)(keys_f32, values_f32, span_total[:, None] - through + input_blocks)
    bw_memory, bw_top = jax.vmap(block_summary)(keys_f32, values_f32, before + input_blocks)
    identity = (jnp.zeros((DQK, DV), jnp.float32), jnp.array(lowest_log, jnp.float32), jnp.array(0.0, jnp.float32))

    def chain_step(running, element):
        return (join_states(running, element), running)
    _, prior_carry = lax.scan(chain_step, identity, (fw_memory, fw_top, span_total))
    _, later_carry = lax.scan(chain_step, identity, (bw_memory, bw_top, span_total), reverse=True)

    def one_block(pieces):
        return block_output(*pieces, head_norm_gain)
    gated_rows = lax.map(one_block, (query_blocks, key_blocks, value_blocks, gate_blocks, input_blocks, through, before, span_total, prior_carry[0], prior_carry[1], later_carry[0], later_carry[1]))
    return gated_rows.reshape(blocks * SPAN, DV)

def expert_half(expert_input_tokens, expert_norm_gain, routes, routed_expert_weight, expert_gate_matrix, expert_up_matrix, expert_down_matrix):
    tokens_f32 = expert_input_tokens.astype(jnp.float32)
    centre = lax.optimization_barrier(jnp.mean(tokens_f32, axis=1, keepdims=True))
    spread = lax.optimization_barrier(jnp.mean(jnp.square(tokens_f32 - centre), axis=1, keepdims=True))
    normed = ((tokens_f32 - centre) * lax.rsqrt(spread + layer_eps) * expert_norm_gain).astype(jnp.bfloat16)
    token_count = expert_input_tokens.shape[0]
    flat_expert = routes.reshape(-1).astype(jnp.int32)
    flat_weight = routed_expert_weight.reshape(-1)
    pair_order = jnp.argsort(flat_expert, stable=True).astype(jnp.int32)
    sorted_expert = flat_expert[pair_order]
    counts = lax.optimization_barrier(jnp.sum((flat_expert[None, :] == jnp.arange(EXPERTS, dtype=jnp.int32)[:, None]).astype(jnp.int32), axis=1))
    starts = (jnp.cumsum(counts) - counts).astype(jnp.int32)
    most_rows = CAP * N_EP * N_TP
    padded_order = jnp.concatenate([pair_order, jnp.zeros((most_rows,), jnp.int32)])
    padded_expert = jnp.concatenate([sorted_expert, jnp.full((most_rows,), -1, jnp.int32)])

    def one_expert(output_sum, expert):
        first = starts[expert].astype(jnp.int32)
        pair_index = lax.dynamic_slice(padded_order, (first,), (most_rows,))
        live_slot = (lax.dynamic_slice(padded_expert, (first,), (most_rows,)) == expert).astype(jnp.float32)
        token_rows = (pair_index // TOP).astype(jnp.int32)
        picked = normed[token_rows]
        gate_part = jnp.dot(picked, expert_gate_matrix[expert], preferred_element_type=jnp.float32)
        up_part = jnp.dot(picked, expert_up_matrix[expert], preferred_element_type=jnp.float32)
        hidden = (jax.nn.silu(gate_part) * up_part).astype(jnp.bfloat16)
        expert_rows = jnp.dot(hidden, expert_down_matrix[expert], preferred_element_type=jnp.float32).astype(jnp.bfloat16)
        expert_rows = lax.optimization_barrier(expert_rows).astype(jnp.float32)
        scaled = (flat_weight[pair_index] * live_slot)[:, None] * expert_rows
        return (output_sum.at[token_rows].add(scaled), None)
    output_sum, _ = lax.scan(one_expert, jnp.zeros((token_count, D), jnp.float32), jnp.arange(EXPERTS, dtype=jnp.int32))
    return output_sum.astype(jnp.bfloat16)

def reference(queries, head_key_rows, head_value_rows, output_gate_logits, log_input_gate, forget_gate_logits, extra_log_forget, head_norm_gain, memory_output_matrix, expert_input_tokens, expert_norm_gain, routes, routed_expert_weight, expert_gate_matrix, expert_up_matrix, expert_down_matrix):
    forget_log_value = jax.nn.log_sigmoid(forget_gate_logits) + extra_log_forget
    mixed_sum = jnp.zeros((queries.shape[0], D), jnp.float32)
    for head_index in range(HEADS):
        gated_rows = mixer_head(queries[:, head_index * DQK:(head_index + 1) * DQK], head_key_rows[:, head_index * DQK:(head_index + 1) * DQK], head_value_rows[:, head_index * DV:(head_index + 1) * DV], output_gate_logits[:, head_index * DV:(head_index + 1) * DV], log_input_gate[head_index], forget_log_value[head_index], head_norm_gain[head_index * DV:(head_index + 1) * DV])
        head_part = jnp.dot(gated_rows, memory_output_matrix[head_index * DV:(head_index + 1) * DV], preferred_element_type=jnp.float32).astype(jnp.bfloat16)
        mixed_sum = mixed_sum + lax.optimization_barrier(head_part).astype(jnp.float32)
    expert_out = expert_half(expert_input_tokens, expert_norm_gain, routes, routed_expert_weight, expert_gate_matrix, expert_up_matrix, expert_down_matrix)
    return (mixed_sum.astype(jnp.bfloat16), expert_out)
```

```python
import functools
import math

import jax
import jax.numpy as jnp
from jax import lax
from jax.experimental import pallas as pl
from jax.experimental.pallas import tpu as pltpu
from jax.sharding import PartitionSpec as P

MESH = pl.DeviceIdType.MESH
F32 = jnp.float32
BF16 = jnp.bfloat16

GRP_EP = ("grp", "ep")
GRP_EP_TP = ("grp", "ep", "tp")
EP_TP = ("ep", "tp")

lowest_log = -1e30
norm_eps = 1e-06
layer_eps = 1e-05
cap = 2
cores = 2


def mm(a, b):
    return lax.dot_general(a, b, (((1,), (0,)), ((), ())), preferred_element_type=F32)


def mm_t(a, b):
    return lax.dot_general(a, b, (((1,), (1,)), ((), ())), preferred_element_type=F32)


def mm_split(a, b):
    high = a.astype(BF16)
    low = (a - high.astype(F32)).astype(BF16)
    return mm(high, b) + mm(low, b)


def iota(shape, dim):
    return lax.broadcasted_iota(jnp.int32, shape, dim)


def kernel(
    nz,
    nx,
    groups,
    q_ref,
    k_ref,
    v_ref,
    og_ref,
    in_gate_ref,
    forget_ref,
    extra_ref,
    head_gain_ref,
    tok_ref,
    norm_gain_ref,
    routes_ref,
    weight_ref,
    wout_hbm,
    wg_hbm,
    wu_hbm,
    wd_hbm,
    mix_ref,
    exp_ref,
    wout,
    wg,
    wu,
    wd,
    normed,
    out1,
    in1,
    out2,
    in2,
    hidden,
    res,
    back,
    ret_out,
    ret_in,
    own_state,
    state_out,
    state_in,
    stat_out,
    stat_in,
    chip_state,
    chip_in,
    chip_stat,
    stats,
    scan_out,
    far,
    gated,
    head_part,
    parts_in,
    load_sem,
    pair_s,
    pair_r,
    z_s,
    z_r,
    x_s,
    x_r,
    a_s,
    a_r,
    t_s,
    t_r,
    b_s,
    b_r,
    rs_s,
    rs_r,
    xb_s,
    xb_r,
    zb_s,
    zb_r,
):
    ep = lax.axis_index("ep")
    x = lax.axis_index("tp")
    z = ep // cores
    c = ep % cores
    nr = nx * cores
    r = c * nx + x
    blk = nr * cap
    gs = nz // groups
    half = nz // 2
    tokens, width = tok_ref.shape
    span, dqk = q_ref.shape
    dv = v_ref.shape[1]
    tile = min(512, width)
    hr = dqk // 2 // nz

    def at(z_, c_, x_):
        return {"ep": z_ * cores + c_, "tp": x_}

    def row_dev(r_):
        return at(z, r_ // nx, r_ % nx)

    def offset(p):
        return half - (p + 1) // 2 if p % 2 else (half + p // 2) % nz if p < nz - 1 else 0

    def copy(src, dst, ssem, rsem, dev):
        return pltpu.make_async_remote_copy(
            src_ref=src,
            dst_ref=dst,
            send_sem=ssem,
            recv_sem=rsem,
            device_id=dev,
            device_id_type=MESH,
        )

    loads = [
        pltpu.make_async_copy(wg_hbm.at[0], wg, load_sem.at[0]),
        pltpu.make_async_copy(wu_hbm.at[0], wu, load_sem.at[1]),
        pltpu.make_async_copy(wd_hbm.at[0], wd, load_sem.at[2]),
        pltpu.make_async_copy(wout_hbm, wout, load_sem.at[3]),
    ]
    for load in loads:
        load.start()

    barrier = pltpu.get_barrier_semaphore()
    for i in range(1, nz):
        pl.semaphore_signal(
            barrier, inc=1, device_id=at((z + i) % nz, c, x), device_id_type=MESH
        )
    for i in range(1, nr):
        pl.semaphore_signal(barrier, inc=1, device_id=row_dev((r + i) % nr), device_id_type=MESH)

    t_f32 = tok_ref[...].astype(F32)
    centre = jnp.mean(t_f32, axis=1, keepdims=True)
    t_f32 = t_f32 - centre
    spread = jnp.mean(t_f32 * t_f32, axis=1, keepdims=True)
    normed[...] = (t_f32 * lax.rsqrt(spread + layer_eps) * norm_gain_ref[...]).astype(BF16)

    t0 = iota((tokens, tokens), 0)
    t1 = iota((tokens, tokens), 1)
    e_col = [routes_ref[:, k : k + 1].astype(F32) for k in range(2)]
    e_row = [jnp.sum(jnp.where(t0 == t1, e, 0.0), axis=0, keepdims=True) for e in e_col]

    def place(e, earlier):
        e = e.astype(jnp.int32)
        step = ((e >> int(math.log2(nr))) - z) & (nz - 1)
        p = jnp.where(step < half, 2 * (half - step) - 1, 2 * (step - half))
        return p * blk + (e & (nr - 1)) * cap + earlier.astype(jnp.int32)

    def one_if(mask):
        return jnp.where(mask, 1.0, 0.0)

    place_row, place_col = [], []
    for k in range(2):
        same = (e_col[0] == e_row[k]) | (e_col[1] == e_row[k])
        earlier = jnp.sum(one_if(same & (t0 < t1)), axis=0, keepdims=True)
        place_row.append(place(e_row[k], earlier))
        same = (e_row[0] == e_col[k]) | (e_row[1] == e_col[k])
        earlier = jnp.sum(one_if(same & (t1 < t0)), axis=1, keepdims=True)
        place_col.append(place(e_col[k], earlier))
    rows = iota((nz * blk, tokens), 0)
    pick = one_if((rows == place_row[0]) | (rows == place_row[1])).astype(BF16)
    for n in range(0, width, tile):
        out1[:, :, n : n + tile] = (
            mm(pick, normed[:, n : n + tile]).astype(BF16).reshape(nz, blk, tile)
        )

    pl.semaphore_wait(barrier, nz - 1 + nr - 1)

    sends = []

    def send(*args):
        made = copy(*args)
        made.start()
        sends.append(made)
        return made

    z_copies = [
        send(
            out1.at[p],
            in1.at[p],
            z_s.at[p],
            z_r.at[p],
            at((z + offset(p)) % nz, c, x),
        )
        for p in range(nz - 1)
    ]
    in1[nz - 1] = out1[nz - 1]

    forget = forget_ref[...]
    forget = jnp.minimum(forget, 0.0) - jnp.log1p(jnp.exp(-jnp.abs(forget))) + extra_ref[...]
    in_gate = in_gate_ref[...]
    ti = iota((span, span), 0)
    si = iota((span, span), 1)
    forget_col = jnp.sum(jnp.where(ti == si, forget, 0.0), axis=1, keepdims=True)
    through_row = jnp.sum(jnp.where(ti <= si, forget_col, 0.0), axis=0, keepdims=True)
    through_col = jnp.sum(jnp.where(si <= ti, forget, 0.0), axis=1, keepdims=True)
    before_row = through_row - forget
    before_col = through_col - forget_col
    total = jnp.sum(forget, axis=1, keepdims=True)
    fw_log = total - through_row + in_gate
    bw_log = before_row + in_gate
    fw_top = jnp.max(fw_log, axis=1, keepdims=True)
    bw_top = jnp.max(bw_log, axis=1, keepdims=True)
    keys_t = jnp.transpose(k_ref[...].astype(F32))
    values = v_ref[...]
    own_state[0] = mm_split(keys_t * jnp.exp(fw_log - fw_top), values)
    own_state[1] = mm_split(keys_t * jnp.exp(bw_log - bw_top), values)
    state_out[...] = own_state[...].astype(BF16)
    stat_out[0:1, :] = jnp.broadcast_to(fw_top, (1, 128))
    stat_out[1:2, :] = jnp.broadcast_to(bw_top, (1, 128))
    stat_out[2:3, :] = jnp.broadcast_to(total, (1, 128))
    stat_out[3:8, :] = jnp.zeros((5, 128), F32)
    partner = at(z, 1 - c, x)
    pair_copies = [
        send(state_out, state_in, pair_s.at[0], pair_r.at[0], partner),
        send(stat_out, stat_in, pair_s.at[1], pair_r.at[1], partner),
    ]

    scale = dqk**-0.5
    fw_in = jnp.where(ti >= si, through_col - through_row + in_gate, -jnp.inf)
    bw_in = jnp.where(ti <= si, before_row - before_col + in_gate, -jnp.inf)
    inner_top = jnp.maximum(
        jnp.max(fw_in, axis=1, keepdims=True), jnp.max(bw_in, axis=1, keepdims=True)
    )

    for made in pair_copies:
        made.wait_recv()
    first = c == 0

    def row(ref, i):
        return ref[i : i + 1, :]

    f_own, b_own, t_own = (row(stat_out, i) for i in range(3))
    f_par, b_par, t_par = (row(stat_in, i) for i in range(3))
    f_own_log = f_own + jnp.where(first, t_par, 0.0)
    f_par_log = f_par + jnp.where(first, 0.0, t_own)
    b_own_log = b_own + jnp.where(first, 0.0, t_par)
    b_par_log = b_par + jnp.where(first, t_own, 0.0)
    f_chip = jnp.maximum(f_own_log, f_par_log)
    b_chip = jnp.maximum(b_own_log, b_par_log)
    mine = pl.ds(pl.multiple_of(c * (dqk // 2), dqk // 2), dqk // 2)
    for i, (own_log, par_log, top) in enumerate(
        ((f_own_log, f_par_log, f_chip), (b_own_log, b_par_log, b_chip))
    ):
        joined = (
            jnp.exp(own_log - top)[:, 0:1] * own_state[i, mine, :]
            + jnp.exp(par_log - top)[:, 0:1] * state_in[i, mine, :].astype(F32)
        )
        chip_state[:, i * hr : (i + 1) * hr, :] = joined.astype(BF16).reshape(nz, hr, dv)
    chip_stat[0:1, :] = f_chip
    chip_stat[1:2, :] = b_chip
    chip_stat[2:3, :] = t_own + t_par
    chip_stat[3:8, :] = jnp.zeros((5, 128), F32)
    a_copies = []
    for i in range(1, nz):
        to = (z + i) % nz
        dev = at(to, c, x)
        a_copies.append(send(chip_stat, stats.at[z], t_s.at[i], t_r.at[i], dev))
        a_copies.append(send(chip_state.at[to], chip_in.at[z], a_s.at[i], a_r.at[i], dev))
    chip_in[z] = chip_state[z]
    stats[z] = chip_stat[...]

    ga, gb = iota((gs * blk, gs * blk), 0), iota((gs * blk, gs * blk), 1)
    lc, lg, lr = (int(math.log2(n)) for n in (cap, gs, nr))
    to_row = ga >> (lc + lg)
    to_mem = (ga >> lc) & (gs - 1)
    fwd = one_if(gb == to_mem * blk + to_row * cap + (ga & (cap - 1))).astype(BF16)
    from_mem = ga >> (lc + lr)
    from_row = (ga >> lc) & (nr - 1)
    rev = one_if(gb == from_row * (gs * cap) + from_mem * cap + (ga & (cap - 1))).astype(BF16)

    x_copies = []
    for g in range(groups):
        for p in range(g * gs, min((g + 1) * gs, nz - 1)):
            z_copies[p].wait_recv()
        for n in range(0, width, tile):
            rows_in = in1[g * gs : (g + 1) * gs, :, n : n + tile].reshape(gs * blk, tile)
            out2[g, :, :, n : n + tile] = (
                mm(fwd, rows_in).astype(BF16).reshape(nr, gs * cap, tile)
            )
        for i in range(1, nr):
            to = (r + i) % nr
            x_copies.append(
                send(out2.at[g, to], in2.at[g, i], x_s.at[g, i], x_r.at[g, i], row_dev(to))
            )
        in2[g, 0] = out2[g, r]

    loads[0].wait()
    loads[1].wait()
    loads[2].wait()
    for made in x_copies:
        made.wait_recv()
    n_rows = nz * blk
    fe = wg.shape[1]
    ft = min(256, fe)
    for n in range(0, fe, ft):
        arrived = in2[...].reshape(n_rows, width)
        gate_part = mm(arrived, wg[:, n : n + ft])
        up_part = mm(arrived, wu[:, n : n + ft])
        hidden[:, n : n + ft] = (gate_part * jax.nn.sigmoid(gate_part) * up_part).astype(BF16)
    for n in range(0, width, tile):
        res[:, :, :, n : n + tile] = (
            mm(hidden[...], wd[:, n : n + tile]).astype(BF16).reshape(groups, nr, gs * cap, tile)
        )
    xb_copies = []
    for g in range(groups):
        made = []
        for i in range(1, nr):
            to = (r + nr - i) % nr
            made.append(
                send(res.at[g, i], back.at[g, r], xb_s.at[g, i], xb_r.at[g, i], row_dev(to))
            )
        xb_copies.append(made)
        back[g, r] = res[g, 0]

    for made in a_copies:
        made.wait_recv()
    lanes = [pl.ds(n, 128) for n in range(0, dv, 128)]
    tops = []
    for i, order in ((0, range(nz)), (1, range(nz - 1, -1, -1))):
        top = jnp.full((1, 128), lowest_log, F32)
        my_top = top
        memory = [jnp.zeros((hr, 128), F32) for _ in lanes]
        for w in order:
            my_top = jnp.where(w == z, top, my_top)
            for lane, m in zip(lanes, memory):
                scan_out[w, i * hr : (i + 1) * hr, lane] = m.astype(BF16)
            state_top, state_total = stats[w, i : i + 1, :], stats[w, 2:3, :]
            new_top = jnp.maximum(state_total + top, state_top)
            keep = jnp.exp(state_total + top - new_top)
            take = jnp.exp(state_top - new_top)
            memory = [
                keep * m + take * chip_in[w, i * hr : (i + 1) * hr, lane].astype(F32)
                for lane, m in zip(lanes, memory)
            ]
            top = new_top
        tops.append(my_top[:, 0:1])
    b_copies = []
    for i in range(1, nz):
        to = (z + i) % nz
        b_copies.append(
            send(scan_out.at[to], far.at[c, z], b_s.at[i], b_r.at[i], at(to, c, x))
        )
    far[c, z] = scan_out[z]

    zb_copies = []
    for g in range(groups):
        for made in xb_copies[g]:
            made.wait_recv()
        for n in range(0, width, tile):
            rows_in = back[g, :, :, n : n + tile].reshape(gs * blk, tile)
            ret_out[g * gs : (g + 1) * gs, :, n : n + tile] = (
                mm(rev, rows_in).astype(BF16).reshape(gs, blk, tile)
            )
        for p in range(g * gs, min((g + 1) * gs, nz - 1)):
            zb_copies.append(
                send(
                    ret_out.at[p],
                    ret_in.at[p],
                    zb_s.at[p],
                    zb_r.at[p],
                    at((z + nz - offset(p)) % nz, c, x),
                )
            )
    ret_in[nz - 1] = ret_out[nz - 1]

    for made in b_copies:
        made.wait_recv()
    far_copy = send(far.at[c], far.at[c], pair_s.at[2], pair_r.at[2], partner)
    far_in = copy(far.at[c], far.at[1 - c], pair_s.at[2], pair_r.at[2], partner)
    scores = mm_t(q_ref[...], k_ref[...]) * scale
    t_own, t_par, f_par, b_par = (v[:, 0:1] for v in (t_own, t_par, f_par, b_par))
    rest_col = total - before_col
    prior_log = through_col + (tops[0] + jnp.where(first, 0.0, t_par))
    later_log = rest_col + (tops[1] + jnp.where(first, t_par, 0.0))
    pair_log = jnp.where(first, rest_col + b_par, through_col + f_par)
    row_top = jnp.maximum(
        jnp.maximum(inner_top, prior_log), jnp.maximum(later_log, pair_log)
    )
    weights = jnp.exp(fw_in - row_top) + jnp.exp(bw_in - row_top)
    near = (scores * weights).astype(BF16)
    far_in.wait_recv()
    queries = q_ref[...]

    def far_memory(i):
        return far[:, :, i * hr : (i + 1) * hr, :].reshape(dqk, dv)

    head_rows = mm(near, v_ref[...]) + scale * (
        jnp.exp(prior_log - row_top) * mm(queries, far_memory(0))
        + jnp.exp(later_log - row_top) * mm(queries, far_memory(1))
        + jnp.exp(pair_log - row_top) * mm(queries, state_in[1 - c])
    )
    head_rows = (
        head_rows
        * lax.rsqrt(jnp.mean(head_rows * head_rows, axis=1, keepdims=True) + norm_eps)
        * head_gain_ref[...]
    )
    gated[...] = (jax.nn.sigmoid(og_ref[...].astype(F32)) * head_rows).astype(BF16)
    loads[3].wait()
    for n in range(0, width, tile):
        head_part[:, :, n : n + tile] = (
            mm(gated[...], wout[:, n : n + tile]).astype(BF16).reshape(nx, span // nx, tile)
        )
    rs_copies = []
    for i in range(1, nx):
        to = (x + i) % nx
        rs_copies.append(
            send(head_part.at[to], parts_in.at[i], rs_s.at[i], rs_r.at[i], at(z, c, to))
        )
    for made in rs_copies:
        made.wait_recv()
    for n in range(0, width, tile):
        mixed = head_part[x, :, n : n + tile].astype(F32)
        for i in range(1, nx):
            mixed = mixed + parts_in[i, :, n : n + tile].astype(F32)
        mix_ref[:, n : n + tile] = mixed.astype(BF16)

    places = iota((tokens, nz * blk), 1)
    share = jnp.where(places == place_col[0], weight_ref[:, 0:1], 0.0) + jnp.where(
        places == place_col[1], weight_ref[:, 1:2], 0.0
    )
    for made in zb_copies:
        made.wait_recv()
    for n in range(0, width, tile):
        returned = ret_in[:, :, n : n + tile].reshape(nz * blk, tile)
        exp_ref[:, n : n + tile] = mm_split(share, returned).astype(BF16)

    for made in sends:
        made.wait_send()


def body(
    nz,
    nx,
    queries,
    head_key_rows,
    head_value_rows,
    output_gate_logits,
    log_input_gate,
    forget_gate_logits,
    extra_log_forget,
    head_norm_gain,
    memory_output_matrix,
    expert_input_tokens,
    expert_norm_gain,
    routes,
    routed_expert_weight,
    expert_gate_matrix,
    expert_up_matrix,
    expert_down_matrix,
):
    span, dqk = queries.shape
    dv = head_value_rows.shape[1]
    tokens, width = expert_input_tokens.shape
    fe = expert_gate_matrix.shape[2]
    nr = nx * cores
    blk = nr * cap
    groups = 4 if nz % 4 == 0 else 1
    gs = nz // groups
    hr = dqk // 2 // nz
    vmem = pl.BlockSpec(memory_space=pltpu.VMEM)
    hbm = pl.BlockSpec(memory_space=pl.ANY)
    dma = pltpu.SemaphoreType.DMA
    mixer_out, expert_out = pl.pallas_call(
        functools.partial(kernel, nz, nx, groups),
        out_shape=(
            jax.ShapeDtypeStruct((span // nx, width), BF16),
            jax.ShapeDtypeStruct((tokens, width), BF16),
        ),
        in_specs=[vmem] * 12 + [hbm] * 4,
        out_specs=(vmem, vmem),
        scratch_shapes=[
            pltpu.VMEM((dv, width), BF16),
            pltpu.VMEM((width, fe), BF16),
            pltpu.VMEM((width, fe), BF16),
            pltpu.VMEM((fe, width), BF16),
            pltpu.VMEM((tokens, width), BF16),
            pltpu.VMEM((nz, blk, width), BF16),
            pltpu.VMEM((nz, blk, width), BF16),
            pltpu.VMEM((groups, nr, gs * cap, width), BF16),
            pltpu.VMEM((groups, nr, gs * cap, width), BF16),
            pltpu.VMEM((nz * blk, fe), BF16),
            pltpu.VMEM((groups, nr, gs * cap, width), BF16),
            pltpu.VMEM((groups, nr, gs * cap, width), BF16),
            pltpu.VMEM((nz, blk, width), BF16),
            pltpu.VMEM((nz, blk, width), BF16),
            pltpu.VMEM((2, dqk, dv), F32),
            pltpu.VMEM((2, dqk, dv), BF16),
            pltpu.VMEM((2, dqk, dv), BF16),
            pltpu.VMEM((8, 128), F32),
            pltpu.VMEM((8, 128), F32),
            pltpu.VMEM((nz, 2 * hr, dv), BF16),
            pltpu.VMEM((nz, 2 * hr, dv), BF16),
            pltpu.VMEM((8, 128), F32),
            pltpu.VMEM((nz, 8, 128), F32),
            pltpu.VMEM((nz, 2 * hr, dv), BF16),
            pltpu.VMEM((2, nz, 2 * hr, dv), BF16),
            pltpu.VMEM((span, dv), BF16),
            pltpu.VMEM((nx, span // nx, width), BF16),
            pltpu.VMEM((nx, span // nx, width), BF16),
            dma((4,)),
            dma((3,)),
            dma((3,)),
            dma((nz,)),
            dma((nz,)),
            dma((groups, nr)),
            dma((groups, nr)),
            dma((nz,)),
            dma((nz,)),
            dma((nz,)),
            dma((nz,)),
            dma((nz,)),
            dma((nz,)),
            dma((nx,)),
            dma((nx,)),
            dma((groups, nr)),
            dma((groups, nr)),
            dma((nz,)),
            dma((nz,)),
        ],
        compiler_params=pltpu.CompilerParams(
            collective_id=0, has_side_effects=True, vmem_limit_bytes=60 * 2**20
        ),
        name="layer_step",
    )(
        queries,
        head_key_rows,
        head_value_rows,
        output_gate_logits,
        log_input_gate,
        forget_gate_logits,
        extra_log_forget,
        head_norm_gain.reshape(1, dv),
        expert_input_tokens,
        expert_norm_gain.reshape(1, width),
        routes,
        routed_expert_weight,
        memory_output_matrix,
        expert_gate_matrix,
        expert_up_matrix,
        expert_down_matrix,
    )
    return mixer_out, expert_out


def solution(mesh):
    nz = mesh.shape["ep"] // cores
    return jax.shard_map(
        functools.partial(body, nz, mesh.shape["tp"]),
        mesh=mesh,
        in_specs=(
            P(GRP_EP, "tp"),
            P(GRP_EP, "tp"),
            P(GRP_EP, "tp"),
            P(GRP_EP, "tp"),
            P("tp", GRP_EP),
            P("tp", GRP_EP),
            P("tp", GRP_EP),
            P("tp"),
            P("tp", None),
            P(GRP_EP_TP, None),
            P(),
            P(GRP_EP_TP, None),
            P(GRP_EP_TP, None),
            P(EP_TP, None, None),
            P(EP_TP, None, None),
            P(EP_TP, None, None),
        ),
        out_specs=(P(GRP_EP_TP, None), P(GRP_EP_TP, None)),
        check_vma=False,
    )
```

```python
import functools
import math

import jax
import jax.numpy as jnp
from jax import lax
from jax.experimental import pallas as pl
from jax.experimental.pallas import tpu as pltpu
from jax.sharding import PartitionSpec as P

MESH = pl.DeviceIdType.MESH
F32 = jnp.float32
BF16 = jnp.bfloat16

GRP_EP = ("grp", "ep")
GRP_EP_TP = ("grp", "ep", "tp")
EP_TP = ("ep", "tp")

lowest_log = -1e30
norm_eps = 1e-06
layer_eps = 1e-05
cap = 2
cores = 2


def mm(a, b):
    return lax.dot_general(a, b, (((1,), (0,)), ((), ())), preferred_element_type=F32)


def mm_t(a, b):
    return lax.dot_general(a, b, (((1,), (1,)), ((), ())), preferred_element_type=F32)


def mm_split(a, b):
    high = a.astype(BF16)
    low = (a - high.astype(F32)).astype(BF16)
    return mm(high, b) + mm(low, b)


def iota(shape, dim):
    return lax.broadcasted_iota(jnp.int32, shape, dim)


def kernel(
    nz,
    nx,
    groups,
    q_ref,
    k_ref,
    v_ref,
    og_ref,
    in_gate_ref,
    forget_ref,
    extra_ref,
    head_gain_ref,
    tok_ref,
    norm_gain_ref,
    routes_ref,
    weight_ref,
    wout_hbm,
    wg_hbm,
    wu_hbm,
    wd_hbm,
    mix_ref,
    exp_ref,
    wout,
    wg,
    wu,
    wd,
    normed,
    out1,
    in1,
    out2,
    in2,
    hidden,
    res,
    back,
    ret_out,
    ret_in,
    own_state,
    state_out,
    state_in,
    stat_out,
    stat_in,
    chip_state,
    chip_in,
    chip_stat,
    stats,
    scan_out,
    far,
    gated,
    head_part,
    parts_in,
    load_sem,
    pair_s,
    pair_r,
    z_s,
    z_r,
    x_s,
    x_r,
    a_s,
    a_r,
    t_s,
    t_r,
    b_s,
    b_r,
    rs_s,
    rs_r,
    xb_s,
    xb_r,
    zb_s,
    zb_r,
):
    ep = lax.axis_index("ep")
    x = lax.axis_index("tp")
    z = ep // cores
    c = ep % cores
    nr = nx * cores
    r = c * nx + x
    blk = nr * cap
    gs = nz // groups
    half = nz // 2
    tokens, width = tok_ref.shape
    span, dqk = q_ref.shape
    dv = v_ref.shape[1]
    tile = min(512, width)
    hr = dqk // 2 // nz

    def at(z_, c_, x_):
        return {"ep": z_ * cores + c_, "tp": x_}

    def row_dev(r_):
        return at(z, r_ // nx, r_ % nx)

    def offset(p):
        return half - (p + 1) // 2 if p % 2 else (half + p // 2) % nz if p < nz - 1 else 0

    def copy(src, dst, ssem, rsem, dev):
        return pltpu.make_async_remote_copy(
            src_ref=src,
            dst_ref=dst,
            send_sem=ssem,
            recv_sem=rsem,
            device_id=dev,
            device_id_type=MESH,
        )

    loads = [
        pltpu.make_async_copy(wg_hbm.at[0], wg, load_sem.at[0]),
        pltpu.make_async_copy(wu_hbm.at[0], wu, load_sem.at[1]),
        pltpu.make_async_copy(wd_hbm.at[0], wd, load_sem.at[2]),
        pltpu.make_async_copy(wout_hbm, wout, load_sem.at[3]),
    ]
    for load in loads:
        load.start()

    barrier = pltpu.get_barrier_semaphore()
    for i in range(1, nz):
        pl.semaphore_signal(
            barrier, inc=1, device_id=at((z + i) % nz, c, x), device_id_type=MESH
        )
    for i in range(1, nr):
        pl.semaphore_signal(barrier, inc=1, device_id=row_dev((r + i) % nr), device_id_type=MESH)

    t_f32 = tok_ref[...].astype(F32)
    centre = jnp.mean(t_f32, axis=1, keepdims=True)
    t_f32 = t_f32 - centre
    spread = jnp.mean(t_f32 * t_f32, axis=1, keepdims=True)
    normed[...] = (t_f32 * lax.rsqrt(spread + layer_eps) * norm_gain_ref[...]).astype(BF16)

    t0 = iota((tokens, tokens), 0)
    t1 = iota((tokens, tokens), 1)

    def to_col(row):
        return jnp.sum(jnp.where(t0 == t1, row, 0.0), axis=1, keepdims=True)

    e_row = [routes_ref[k : k + 1, :].astype(F32) for k in range(2)]
    e_col = [to_col(e) for e in e_row]

    def place(e, earlier):
        e = e.astype(jnp.int32)
        step = ((e >> int(math.log2(nr))) - z) & (nz - 1)
        p = jnp.where(step < half, 2 * (half - step) - 1, 2 * (step - half))
        return p * blk + (e & (nr - 1)) * cap + earlier.astype(jnp.int32)

    def one_if(mask):
        return jnp.where(mask, 1.0, 0.0)

    place_row, place_col = [], []
    for k in range(2):
        same = (e_col[0] == e_row[k]) | (e_col[1] == e_row[k])
        earlier = jnp.sum(one_if(same & (t0 < t1)), axis=0, keepdims=True)
        place_row.append(place(e_row[k], earlier))
        same = (e_row[0] == e_col[k]) | (e_row[1] == e_col[k])
        earlier = jnp.sum(one_if(same & (t1 < t0)), axis=1, keepdims=True)
        place_col.append(place(e_col[k], earlier))
    rows = iota((nz * blk, tokens), 0)
    pick = one_if((rows == place_row[0]) | (rows == place_row[1])).astype(BF16)
    for n in range(0, width, tile):
        out1[:, :, n : n + tile] = (
            mm(pick, normed[:, n : n + tile]).astype(BF16).reshape(nz, blk, tile)
        )

    pl.semaphore_wait(barrier, nz - 1 + nr - 1)

    sends = []

    def send(*args):
        made = copy(*args)
        made.start()
        sends.append(made)
        return made

    def z_send(places):
        return [
            send(
                out1.at[p],
                in1.at[p],
                z_s.at[p],
                z_r.at[p],
                at((z + offset(p)) % nz, c, x),
            )
            for p in places
        ]

    z_copies = z_send(range(min(gs, nz - 1)))
    in1[nz - 1] = out1[nz - 1]

    forget = forget_ref[...]
    forget = jnp.minimum(forget, 0.0) - jnp.log1p(jnp.exp(-jnp.abs(forget))) + extra_ref[...]
    in_gate = in_gate_ref[...]
    ti = iota((span, span), 0)
    si = iota((span, span), 1)
    forget_col = jnp.sum(jnp.where(ti == si, forget, 0.0), axis=1, keepdims=True)
    through_row = jnp.sum(jnp.where(ti <= si, forget_col, 0.0), axis=0, keepdims=True)
    through_col = jnp.sum(jnp.where(si <= ti, forget, 0.0), axis=1, keepdims=True)
    before_row = through_row - forget
    before_col = through_col - forget_col
    total = jnp.sum(forget, axis=1, keepdims=True)
    fw_log = total - through_row + in_gate
    bw_log = before_row + in_gate
    fw_top = jnp.max(fw_log, axis=1, keepdims=True)
    bw_top = jnp.max(bw_log, axis=1, keepdims=True)
    keys_t = jnp.transpose(k_ref[...].astype(F32))
    values = v_ref[...]
    own_state[0] = mm_split(keys_t * jnp.exp(fw_log - fw_top), values)
    own_state[1] = mm_split(keys_t * jnp.exp(bw_log - bw_top), values)
    state_out[...] = own_state[...].astype(BF16)
    stat_out[0:1, :] = jnp.broadcast_to(fw_top, (1, 128))
    stat_out[1:2, :] = jnp.broadcast_to(bw_top, (1, 128))
    stat_out[2:3, :] = jnp.broadcast_to(total, (1, 128))
    stat_out[3:8, :] = jnp.zeros((5, 128), F32)
    partner = at(z, 1 - c, x)
    pair_copies = [
        send(state_out, state_in, pair_s.at[0], pair_r.at[0], partner),
        send(stat_out, stat_in, pair_s.at[1], pair_r.at[1], partner),
    ]

    scale = dqk**-0.5
    fw_in = jnp.where(ti >= si, through_col - through_row + in_gate, -jnp.inf)
    bw_in = jnp.where(ti <= si, before_row - before_col + in_gate, -jnp.inf)
    inner_top = jnp.maximum(
        jnp.max(fw_in, axis=1, keepdims=True), jnp.max(bw_in, axis=1, keepdims=True)
    )

    for made in pair_copies:
        made.wait_recv()
    first = c == 0

    def row(ref, i):
        return ref[i : i + 1, :]

    f_own, b_own, t_own = (row(stat_out, i) for i in range(3))
    f_par, b_par, t_par = (row(stat_in, i) for i in range(3))
    f_own_log = f_own + jnp.where(first, t_par, 0.0)
    f_par_log = f_par + jnp.where(first, 0.0, t_own)
    b_own_log = b_own + jnp.where(first, 0.0, t_par)
    b_par_log = b_par + jnp.where(first, t_own, 0.0)
    f_chip = jnp.maximum(f_own_log, f_par_log)
    b_chip = jnp.maximum(b_own_log, b_par_log)
    mine = pl.ds(pl.multiple_of(c * (dqk // 2), dqk // 2), dqk // 2)
    for i, (own_log, par_log, top) in enumerate(
        ((f_own_log, f_par_log, f_chip), (b_own_log, b_par_log, b_chip))
    ):
        joined = (
            jnp.exp(own_log - top)[:, 0:1] * own_state[i, mine, :]
            + jnp.exp(par_log - top)[:, 0:1] * state_in[i, mine, :].astype(F32)
        )
        chip_state[:, i * hr : (i + 1) * hr, :] = joined.astype(BF16).reshape(nz, hr, dv)
    chip_stat[0:1, :] = f_chip
    chip_stat[1:2, :] = b_chip
    chip_stat[2:3, :] = t_own + t_par
    chip_stat[3:8, :] = jnp.zeros((5, 128), F32)
    a_copies = []
    for i in range(1, nz):
        to = (z + i) % nz
        dev = at(to, c, x)
        a_copies.append(send(chip_stat, stats.at[z], t_s.at[i], t_r.at[i], dev))
        a_copies.append(send(chip_state.at[to], chip_in.at[z], a_s.at[i], a_r.at[i], dev))
    z_copies += z_send(range(min(gs, nz - 1), nz - 1))
    chip_in[z] = chip_state[z]
    stats[z] = chip_stat[...]

    ga, gb = iota((gs * blk, gs * blk), 0), iota((gs * blk, gs * blk), 1)
    lc, lg, lr = (int(math.log2(n)) for n in (cap, gs, nr))
    to_row = ga >> (lc + lg)
    to_mem = (ga >> lc) & (gs - 1)
    fwd = one_if(gb == to_mem * blk + to_row * cap + (ga & (cap - 1))).astype(BF16)
    from_mem = ga >> (lc + lr)
    from_row = (ga >> lc) & (nr - 1)
    rev = one_if(gb == from_row * (gs * cap) + from_mem * cap + (ga & (cap - 1))).astype(BF16)

    x_copies, xb_copies, zb_copies = [], [], []
    n_rows = gs * blk
    fe = wg.shape[1]
    ft = min(256, fe)

    def spread(g):
        for p in range(g * gs, min((g + 1) * gs, nz - 1)):
            z_copies[p].wait_recv()
        for n in range(0, width, tile):
            rows_in = in1[g * gs : (g + 1) * gs, :, n : n + tile].reshape(n_rows, tile)
            out2[g, :, :, n : n + tile] = (
                mm(fwd, rows_in).astype(BF16).reshape(nr, gs * cap, tile)
            )
        made = []
        for i in range(1, nr):
            to = (r + i) % nr
            made.append(
                send(out2.at[g, to], in2.at[g, i], x_s.at[g, i], x_r.at[g, i], row_dev(to))
            )
        x_copies.append(made)
        in2[g, 0] = out2[g, r]

    def experts(g):
        for made in x_copies[g]:
            made.wait_recv()
        for n in range(0, fe, ft):
            arrived = in2[g].reshape(n_rows, width)
            gate_part = mm(arrived, wg[:, n : n + ft])
            up_part = mm(arrived, wu[:, n : n + ft])
            hidden[:, n : n + ft] = (gate_part * jax.nn.sigmoid(gate_part) * up_part).astype(BF16)
        for n in range(0, width, tile):
            res[g, :, :, n : n + tile] = (
                mm(hidden[...], wd[:, n : n + tile]).astype(BF16).reshape(nr, gs * cap, tile)
            )
        made = []
        for i in range(1, nr):
            to = (r + nr - i) % nr
            made.append(
                send(res.at[g, i], back.at[g, r], xb_s.at[g, i], xb_r.at[g, i], row_dev(to))
            )
        xb_copies.append(made)
        back[g, r] = res[g, 0]

    def give_back(g):
        for made in xb_copies[g]:
            made.wait_recv()
        for n in range(0, width, tile):
            rows_in = back[g, :, :, n : n + tile].reshape(n_rows, tile)
            ret_out[g * gs : (g + 1) * gs, :, n : n + tile] = (
                mm(rev, rows_in).astype(BF16).reshape(gs, blk, tile)
            )
        for p in range(g * gs, min((g + 1) * gs, nz - 1)):
            zb_copies.append(
                send(
                    ret_out.at[p],
                    ret_in.at[p],
                    zb_s.at[p],
                    zb_r.at[p],
                    at((z + nz - offset(p)) % nz, c, x),
                )
            )

    spread(0)

    for made in a_copies:
        made.wait_recv()
    lanes = [pl.ds(n, 128) for n in range(0, dv, 128)]
    tops = []
    for i, order in ((0, range(nz)), (1, range(nz - 1, -1, -1))):
        top = jnp.full((1, 128), lowest_log, F32)
        my_top = top
        memory = [jnp.zeros((hr, 128), F32) for _ in lanes]
        for w in order:
            my_top = jnp.where(w == z, top, my_top)
            for lane, m in zip(lanes, memory):
                scan_out[w, i * hr : (i + 1) * hr, lane] = m.astype(BF16)
            state_top, state_total = stats[w, i : i + 1, :], stats[w, 2:3, :]
            new_top = jnp.maximum(state_total + top, state_top)
            keep = jnp.exp(state_total + top - new_top)
            take = jnp.exp(state_top - new_top)
            memory = [
                keep * m + take * chip_in[w, i * hr : (i + 1) * hr, lane].astype(F32)
                for lane, m in zip(lanes, memory)
            ]
            top = new_top
        tops.append(my_top[:, 0:1])
    b_copies = []
    for i in range(1, nz):
        to = (z + i) % nz
        b_copies.append(
            send(scan_out.at[to], far.at[c, z], b_s.at[i], b_r.at[i], at(to, c, x))
        )
    far[c, z] = scan_out[z]

    for load in loads[:3]:
        load.wait()
    for g in range(1, groups + 2):
        if g < groups:
            spread(g)
        if 0 <= g - 1 < groups:
            experts(g - 1)
        if 0 <= g - 2 < groups:
            give_back(g - 2)
    ret_in[nz - 1] = ret_out[nz - 1]

    for made in b_copies:
        made.wait_recv()
    far_copy = send(far.at[c], far.at[c], pair_s.at[2], pair_r.at[2], partner)
    far_in = copy(far.at[c], far.at[1 - c], pair_s.at[2], pair_r.at[2], partner)
    scores = mm_t(q_ref[...], k_ref[...]) * scale
    t_own, t_par, f_par, b_par = (v[:, 0:1] for v in (t_own, t_par, f_par, b_par))
    rest_col = total - before_col
    prior_log = through_col + (tops[0] + jnp.where(first, 0.0, t_par))
    later_log = rest_col + (tops[1] + jnp.where(first, t_par, 0.0))
    pair_log = jnp.where(first, rest_col + b_par, through_col + f_par)
    row_top = jnp.maximum(
        jnp.maximum(inner_top, prior_log), jnp.maximum(later_log, pair_log)
    )
    weights = jnp.exp(fw_in - row_top) + jnp.exp(bw_in - row_top)
    near = (scores * weights).astype(BF16)
    far_in.wait_recv()
    queries = q_ref[...]

    def far_memory(i):
        return far[:, :, i * hr : (i + 1) * hr, :].reshape(dqk, dv)

    head_rows = mm(near, v_ref[...]) + scale * (
        jnp.exp(prior_log - row_top) * mm(queries, far_memory(0))
        + jnp.exp(later_log - row_top) * mm(queries, far_memory(1))
        + jnp.exp(pair_log - row_top) * mm(queries, state_in[1 - c])
    )
    head_rows = (
        head_rows
        * lax.rsqrt(jnp.mean(head_rows * head_rows, axis=1, keepdims=True) + norm_eps)
        * head_gain_ref[...]
    )
    gated[...] = (jax.nn.sigmoid(og_ref[...].astype(F32)) * head_rows).astype(BF16)
    loads[3].wait()
    for n in range(0, width, tile):
        head_part[:, :, n : n + tile] = (
            mm(gated[...], wout[:, n : n + tile]).astype(BF16).reshape(nx, span // nx, tile)
        )
    rs_copies = []
    for i in range(1, nx):
        to = (x + i) % nx
        rs_copies.append(
            send(head_part.at[to], parts_in.at[i], rs_s.at[i], rs_r.at[i], at(z, c, to))
        )
    for made in rs_copies:
        made.wait_recv()
    for n in range(0, width, tile):
        mixed = head_part[x, :, n : n + tile].astype(F32)
        for i in range(1, nx):
            mixed = mixed + parts_in[i, :, n : n + tile].astype(F32)
        mix_ref[:, n : n + tile] = mixed.astype(BF16)

    places = iota((tokens, nz * blk), 1)
    share = jnp.where(places == place_col[0], to_col(weight_ref[0:1, :]), 0.0) + jnp.where(
        places == place_col[1], to_col(weight_ref[1:2, :]), 0.0
    )
    for made in zb_copies:
        made.wait_recv()
    for n in range(0, width, tile):
        returned = ret_in[:, :, n : n + tile].reshape(nz * blk, tile)
        exp_ref[:, n : n + tile] = mm_split(share, returned).astype(BF16)

    for made in sends:
        made.wait_send()


def body(
    nz,
    nx,
    queries,
    head_key_rows,
    head_value_rows,
    output_gate_logits,
    log_input_gate,
    forget_gate_logits,
    extra_log_forget,
    head_norm_gain,
    memory_output_matrix,
    expert_input_tokens,
    expert_norm_gain,
    routes,
    routed_expert_weight,
    expert_gate_matrix,
    expert_up_matrix,
    expert_down_matrix,
):
    span, dqk = queries.shape
    dv = head_value_rows.shape[1]
    tokens, width = expert_input_tokens.shape
    fe = expert_gate_matrix.shape[2]
    nr = nx * cores
    blk = nr * cap
    groups = 4 if nz % 4 == 0 else 1
    gs = nz // groups
    hr = dqk // 2 // nz
    vmem = pl.BlockSpec(memory_space=pltpu.VMEM)
    hbm = pl.BlockSpec(memory_space=pl.ANY)
    dma = pltpu.SemaphoreType.DMA
    mixer_out, expert_out = pl.pallas_call(
        functools.partial(kernel, nz, nx, groups),
        out_shape=(
            jax.ShapeDtypeStruct((span // nx, width), BF16),
            jax.ShapeDtypeStruct((tokens, width), BF16),
        ),
        in_specs=[vmem] * 12 + [hbm] * 4,
        out_specs=(vmem, vmem),
        scratch_shapes=[
            pltpu.VMEM((dv, width), BF16),
            pltpu.VMEM((width, fe), BF16),
            pltpu.VMEM((width, fe), BF16),
            pltpu.VMEM((fe, width), BF16),
            pltpu.VMEM((tokens, width), BF16),
            pltpu.VMEM((nz, blk, width), BF16),
            pltpu.VMEM((nz, blk, width), BF16),
            pltpu.VMEM((groups, nr, gs * cap, width), BF16),
            pltpu.VMEM((groups, nr, gs * cap, width), BF16),
            pltpu.VMEM((gs * blk, fe), BF16),
            pltpu.VMEM((groups, nr, gs * cap, width), BF16),
            pltpu.VMEM((groups, nr, gs * cap, width), BF16),
            pltpu.VMEM((nz, blk, width), BF16),
            pltpu.VMEM((nz, blk, width), BF16),
            pltpu.VMEM((2, dqk, dv), F32),
            pltpu.VMEM((2, dqk, dv), BF16),
            pltpu.VMEM((2, dqk, dv), BF16),
            pltpu.VMEM((8, 128), F32),
            pltpu.VMEM((8, 128), F32),
            pltpu.VMEM((nz, 2 * hr, dv), BF16),
            pltpu.VMEM((nz, 2 * hr, dv), BF16),
            pltpu.VMEM((8, 128), F32),
            pltpu.VMEM((nz, 8, 128), F32),
            pltpu.VMEM((nz, 2 * hr, dv), BF16),
            pltpu.VMEM((2, nz, 2 * hr, dv), BF16),
            pltpu.VMEM((span, dv), BF16),
            pltpu.VMEM((nx, span // nx, width), BF16),
            pltpu.VMEM((nx, span // nx, width), BF16),
            dma((4,)),
            dma((3,)),
            dma((3,)),
            dma((nz,)),
            dma((nz,)),
            dma((groups, nr)),
            dma((groups, nr)),
            dma((nz,)),
            dma((nz,)),
            dma((nz,)),
            dma((nz,)),
            dma((nz,)),
            dma((nz,)),
            dma((nx,)),
            dma((nx,)),
            dma((groups, nr)),
            dma((groups, nr)),
            dma((nz,)),
            dma((nz,)),
        ],
        compiler_params=pltpu.CompilerParams(
            collective_id=0, has_side_effects=True, vmem_limit_bytes=60 * 2**20
        ),
        name="layer_step",
    )(
        queries,
        head_key_rows,
        head_value_rows,
        output_gate_logits,
        log_input_gate,
        forget_gate_logits,
        extra_log_forget,
        head_norm_gain.reshape(1, dv),
        expert_input_tokens,
        expert_norm_gain.reshape(1, width),
        routes.T,
        routed_expert_weight.T,
        memory_output_matrix,
        expert_gate_matrix,
        expert_up_matrix,
        expert_down_matrix,
    )
    return mixer_out, expert_out


def solution(mesh):
    nz = mesh.shape["ep"] // cores
    return jax.shard_map(
        functools.partial(body, nz, mesh.shape["tp"]),
        mesh=mesh,
        in_specs=(
            P(GRP_EP, "tp"),
            P(GRP_EP, "tp"),
            P(GRP_EP, "tp"),
            P(GRP_EP, "tp"),
            P("tp", GRP_EP),
            P("tp", GRP_EP),
            P("tp", GRP_EP),
            P("tp"),
            P("tp", None),
            P(GRP_EP_TP, None),
            P(),
            P(GRP_EP_TP, None),
            P(GRP_EP_TP, None),
            P(EP_TP, None, None),
            P(EP_TP, None, None),
            P(EP_TP, None, None),
        ),
        out_specs=(P(GRP_EP_TP, None), P(GRP_EP_TP, None)),
        check_vma=False,
    )
```

```python
import functools
import math

import jax
import jax.numpy as jnp
from jax import lax
from jax.experimental import pallas as pl
from jax.experimental.pallas import tpu as pltpu
from jax.sharding import PartitionSpec as P

MESH = pl.DeviceIdType.MESH
F32 = jnp.float32
BF16 = jnp.bfloat16

GRP_EP = ("grp", "ep")
GRP_EP_TP = ("grp", "ep", "tp")
EP_TP = ("ep", "tp")

lowest_log = -1e30
norm_eps = 1e-06
layer_eps = 1e-05
cap = 2
cores = 2


def mm(a, b):
    return lax.dot_general(a, b, (((1,), (0,)), ((), ())), preferred_element_type=F32)


def mm_t(a, b):
    return lax.dot_general(a, b, (((1,), (1,)), ((), ())), preferred_element_type=F32)


def mm_split(a, b):
    high = a.astype(BF16)
    low = (a - high.astype(F32)).astype(BF16)
    return mm(high, b) + mm(low, b)


def iota(shape, dim):
    return lax.broadcasted_iota(jnp.int32, shape, dim)


def kernel(
    nz,
    nx,
    groups,
    in_gate_hbm,
    forget_hbm,
    extra_hbm,
    head_gain_hbm,
    norm_gain_hbm,
    routes_hbm,
    weight_hbm,
    tok_hbm,
    k_hbm,
    v_hbm,
    q_hbm,
    og_hbm,
    wout_hbm,
    wg_hbm,
    wu_hbm,
    wd_hbm,
    mix_ref,
    exp_ref,
    in_gate_ref,
    forget_ref,
    extra_ref,
    head_gain_ref,
    norm_gain_ref,
    routes_ref,
    weight_ref,
    tok_ref,
    k_ref,
    v_ref,
    q_ref,
    og_ref,
    wout,
    wg,
    wu,
    wd,
    normed,
    out1,
    in1,
    out2,
    in2,
    hidden,
    res,
    back,
    ret_out,
    ret_in,
    own_state,
    state_out,
    state_in,
    stat_out,
    stat_in,
    own_chip,
    chip_state,
    chip_stat,
    near_state,
    near_stat,
    pair_state,
    pair_stat,
    pairs_in,
    stats,
    scan_out,
    top_out,
    top_in,
    far,
    gated,
    head_part,
    parts_in,
    partial,
    load_sem,
    pair_s,
    pair_r,
    n_s,
    n_r,
    z_s,
    z_r,
    x_s,
    x_r,
    a_s,
    a_r,
    t_s,
    t_r,
    b_s,
    b_r,
    rs_s,
    rs_r,
    xb_s,
    xb_r,
    zb_s,
    zb_r,
):
    ep = lax.axis_index("ep")
    x = lax.axis_index("tp")
    z = ep // cores
    c = ep % cores
    nr = nx * cores
    r = c * nx + x
    blk = nr * cap
    gs = nz // groups
    half = nz // 2
    tokens, width = tok_ref.shape
    span, dqk = q_ref.shape
    dv = v_ref.shape[1]
    tile = min(512, width)
    hr = dqk // 2 // (nz // 2)

    def at(z_, c_, x_):
        return {"ep": z_ * cores + c_, "tp": x_}

    def row_dev(r_):
        return at(z, r_ // nx, r_ % nx)

    def offset(p):
        return half - (p + 1) // 2 if p % 2 else (half + p // 2) % nz if p < nz - 1 else 0

    def copy(src, dst, ssem, rsem, dev):
        return pltpu.make_async_remote_copy(
            src_ref=src,
            dst_ref=dst,
            send_sem=ssem,
            recv_sem=rsem,
            device_id=dev,
            device_id_type=MESH,
        )

    first_loads = [
        pltpu.make_async_copy(src, dst, load_sem.at[4 + i])
        for i, (src, dst) in enumerate(
            (
                (tok_hbm, tok_ref),
                (routes_hbm, routes_ref),
                (norm_gain_hbm, norm_gain_ref),
                (in_gate_hbm, in_gate_ref),
                (forget_hbm, forget_ref),
                (extra_hbm, extra_ref),
                (k_hbm, k_ref),
                (v_hbm, v_ref),
                (q_hbm, q_ref),
                (og_hbm, og_ref),
                (head_gain_hbm, head_gain_ref),
                (weight_hbm, weight_ref),
            )
        )
    ]
    loads = [
        pltpu.make_async_copy(wg_hbm.at[0], wg, load_sem.at[0]),
        pltpu.make_async_copy(wu_hbm.at[0], wu, load_sem.at[1]),
        pltpu.make_async_copy(wd_hbm.at[0], wd, load_sem.at[2]),
        pltpu.make_async_copy(wout_hbm, wout, load_sem.at[3]),
    ]
    barrier = pltpu.get_barrier_semaphore()
    for i in range(1, nz):
        pl.semaphore_signal(
            barrier, inc=1, device_id=at((z + i) % nz, c, x), device_id_type=MESH
        )
    for i in range(1, nr):
        pl.semaphore_signal(barrier, inc=1, device_id=row_dev((r + i) % nr), device_id_type=MESH)

    for load in first_loads + loads:
        load.start()

    for load in first_loads[:3]:
        load.wait()
    t_f32 = tok_ref[...].astype(F32)
    centre = jnp.mean(t_f32, axis=1, keepdims=True)
    t_f32 = t_f32 - centre
    spread = jnp.mean(t_f32 * t_f32, axis=1, keepdims=True)
    normed[...] = (t_f32 * lax.rsqrt(spread + layer_eps) * norm_gain_ref[...]).astype(BF16)

    t0 = iota((tokens, tokens), 0)
    t1 = iota((tokens, tokens), 1)

    def to_col(row):
        return jnp.sum(jnp.where(t0 == t1, row, 0.0), axis=1, keepdims=True)

    e_row = [routes_ref[k : k + 1, :].astype(F32) for k in range(2)]
    e_col = [to_col(e) for e in e_row]

    def place(e, earlier):
        e = e.astype(jnp.int32)
        step = ((e >> int(math.log2(nr))) - z) & (nz - 1)
        p = jnp.where(step < half, 2 * (half - step) - 1, 2 * (step - half))
        return p * blk + (e & (nr - 1)) * cap + earlier.astype(jnp.int32)

    def one_if(mask):
        return jnp.where(mask, 1.0, 0.0)

    place_row, place_col = [], []
    for k in range(2):
        same = (e_col[0] == e_row[k]) | (e_col[1] == e_row[k])
        earlier = jnp.sum(one_if(same & (t0 < t1)), axis=0, keepdims=True)
        place_row.append(place(e_row[k], earlier))
        same = (e_row[0] == e_col[k]) | (e_row[1] == e_col[k])
        earlier = jnp.sum(one_if(same & (t1 < t0)), axis=1, keepdims=True)
        place_col.append(place(e_col[k], earlier))
    rows = iota((nz * blk, tokens), 0)
    pick = one_if((rows == place_row[0]) | (rows == place_row[1])).astype(BF16)
    for n in range(0, width, tile):
        out1[:, :, n : n + tile] = (
            mm(pick, normed[:, n : n + tile]).astype(BF16).reshape(nz, blk, tile)
        )

    for load in first_loads[3:8]:
        load.wait()
    forget = forget_ref[...]
    forget = jnp.minimum(forget, 0.0) - jnp.log1p(jnp.exp(-jnp.abs(forget))) + extra_ref[...]
    in_gate = in_gate_ref[...]
    ti = iota((span, span), 0)
    si = iota((span, span), 1)
    forget_col = jnp.sum(jnp.where(ti == si, forget, 0.0), axis=1, keepdims=True)
    through_row = jnp.sum(jnp.where(ti <= si, forget_col, 0.0), axis=0, keepdims=True)
    through_col = jnp.sum(jnp.where(si <= ti, forget, 0.0), axis=1, keepdims=True)
    before_row = through_row - forget
    before_col = through_col - forget_col
    total = jnp.sum(forget, axis=1, keepdims=True)
    fw_log = total - through_row + in_gate
    bw_log = before_row + in_gate
    fw_top = jnp.max(fw_log, axis=1, keepdims=True)
    bw_top = jnp.max(bw_log, axis=1, keepdims=True)
    keys_t = jnp.transpose(k_ref[...].astype(F32))
    values = v_ref[...]
    own_state[0] = mm_split(keys_t * jnp.exp(fw_log - fw_top), values)
    own_state[1] = mm_split(keys_t * jnp.exp(bw_log - bw_top), values)
    state_out[...] = own_state[...].astype(BF16)
    stat_out[0:1, :] = jnp.broadcast_to(fw_top, (1, 128))
    stat_out[1:2, :] = jnp.broadcast_to(bw_top, (1, 128))
    stat_out[2:3, :] = jnp.broadcast_to(total, (1, 128))
    stat_out[3:8, :] = jnp.zeros((5, 128), F32)
    pl.semaphore_wait(barrier, nz - 1 + nr - 1)

    sends = []

    def send(*args):
        made = copy(*args)
        made.start()
        sends.append(made)
        return made

    def z_send(places):
        return [
            send(
                out1.at[p],
                in1.at[p],
                z_s.at[p],
                z_r.at[p],
                at((z + offset(p)) % nz, c, x),
            )
            for p in places
        ]


    partner = at(z, 1 - c, x)
    pair_copies = [
        send(state_out, state_in, pair_s.at[0], pair_r.at[0], partner),
        send(stat_out, stat_in, pair_s.at[1], pair_r.at[1], partner),
    ]

    z_copies = z_send(range(1))
    in1[nz - 1] = out1[nz - 1]

    scale = dqk**-0.5
    fw_in = jnp.where(ti >= si, through_col - through_row + in_gate, -jnp.inf)
    bw_in = jnp.where(ti <= si, before_row - before_col + in_gate, -jnp.inf)
    inner_top = jnp.maximum(
        jnp.max(fw_in, axis=1, keepdims=True), jnp.max(bw_in, axis=1, keepdims=True)
    )

    for made in pair_copies:
        made.wait_recv()
    first = c == 0

    def row(ref, i):
        return ref[i : i + 1, :]

    f_own, b_own, t_own = (row(stat_out, i) for i in range(3))
    f_par, b_par, t_par = (row(stat_in, i) for i in range(3))
    f_own_log = f_own + jnp.where(first, t_par, 0.0)
    f_par_log = f_par + jnp.where(first, 0.0, t_own)
    b_own_log = b_own + jnp.where(first, 0.0, t_par)
    b_par_log = b_par + jnp.where(first, t_own, 0.0)
    f_chip = jnp.maximum(f_own_log, f_par_log)
    b_chip = jnp.maximum(b_own_log, b_par_log)
    mine = pl.ds(pl.multiple_of(c * (dqk // 2), dqk // 2), dqk // 2)
    for i, (own_log, par_log, top) in enumerate(
        ((f_own_log, f_par_log, f_chip), (b_own_log, b_par_log, b_chip))
    ):
        joined = (
            jnp.exp(own_log - top)[:, 0:1] * own_state[i, mine, :]
            + jnp.exp(par_log - top)[:, 0:1] * state_in[i, mine, :].astype(F32)
        )
        own_chip[i] = joined
        chip_state[i] = joined.astype(BF16)
    t_chip = t_own + t_par
    chip_stat[0:1, :] = f_chip
    chip_stat[1:2, :] = b_chip
    chip_stat[2:3, :] = t_chip
    chip_stat[3:8, :] = jnp.zeros((5, 128), F32)

    odd = z % 2
    later = odd == 1
    m = z // 2
    neighbour = at(z + 1 - 2 * odd, c, x)
    n_pairs = nz // 2
    next_copies = [
        send(chip_stat, near_stat, n_s.at[0], n_r.at[0], neighbour),
        send(chip_state.at[odd], near_state.at[c], n_s.at[1], n_r.at[1], neighbour),
    ]
    z_copies += z_send(range(1, min(gs, nz - 1)))
    for made in next_copies:
        made.wait_recv()
    f_near, b_near, t_near = (row(near_stat, i) for i in range(3))
    own_log = jnp.where(later, f_chip, b_chip)
    near_log = jnp.where(later, f_near, b_near) + t_chip
    pair_top = jnp.maximum(own_log, near_log)
    joined = (
        jnp.exp(own_log - pair_top)[:, 0:1] * own_chip[1 - odd]
        + jnp.exp(near_log - pair_top)[:, 0:1] * near_state[c].astype(F32)
    )
    pair_state[...] = joined.astype(BF16).reshape(n_pairs, hr, dv)
    pair_stat[0:1, :] = pair_top
    pair_stat[1:2, :] = t_chip + t_near
    pair_stat[2:8, :] = jnp.zeros((6, 128), F32)
    a_copies = []
    for i in range(1, n_pairs):
        to = (m + i) % n_pairs
        dev = at(2 * to + odd, c, x)
        a_copies.append(send(pair_stat, stats.at[m], t_s.at[i], t_r.at[i], dev))
        a_copies.append(send(pair_state.at[to], pairs_in.at[m], a_s.at[i], a_r.at[i], dev))
    z_copies += z_send(range(min(gs, nz - 1), min(2 * gs, nz - 1)))
    pairs_in[m] = pair_state[m]
    stats[m] = pair_stat[...]

    ga, gb = iota((gs * blk, gs * blk), 0), iota((gs * blk, gs * blk), 1)
    lc, lg, lr = (int(math.log2(n)) for n in (cap, gs, nr))
    to_row = ga >> (lc + lg)
    to_mem = (ga >> lc) & (gs - 1)
    fwd = one_if(gb == to_mem * blk + to_row * cap + (ga & (cap - 1))).astype(BF16)
    from_mem = ga >> (lc + lr)
    from_row = (ga >> lc) & (nr - 1)
    rev = one_if(gb == from_row * (gs * cap) + from_mem * cap + (ga & (cap - 1))).astype(BF16)

    x_copies, xb_copies, zb_copies = [], [], []
    n_rows = gs * blk
    fe = wg.shape[1]
    ft = min(256, fe)

    def spread(g):
        for p in range(g * gs, min((g + 1) * gs, nz - 1)):
            z_copies[p].wait_recv()
        for n in range(0, width, tile):
            rows_in = in1[g * gs : (g + 1) * gs, :, n : n + tile].reshape(n_rows, tile)
            out2[g, :, :, n : n + tile] = (
                mm(fwd, rows_in).astype(BF16).reshape(nr, gs * cap, tile)
            )
        made = []
        for i in range(1, nr):
            to = (r + i) % nr
            made.append(
                send(out2.at[g, to], in2.at[g, i], x_s.at[g, i], x_r.at[g, i], row_dev(to))
            )
        x_copies.append(made)
        in2[g, 0] = out2[g, r]

    def experts(g):
        for made in x_copies[g]:
            made.wait_recv()
        for n in range(0, fe, ft):
            arrived = in2[g].reshape(n_rows, width)
            gate_part = mm(arrived, wg[:, n : n + ft])
            up_part = mm(arrived, wu[:, n : n + ft])
            hidden[:, n : n + ft] = (gate_part * jax.nn.sigmoid(gate_part) * up_part).astype(BF16)
        for n in range(0, width, tile):
            res[g, :, :, n : n + tile] = (
                mm(hidden[...], wd[:, n : n + tile]).astype(BF16).reshape(nr, gs * cap, tile)
            )
        made = []
        for i in range(1, nr):
            to = (r + nr - i) % nr
            made.append(
                send(res.at[g, i], back.at[g, r], xb_s.at[g, i], xb_r.at[g, i], row_dev(to))
            )
        xb_copies.append(made)
        back[g, r] = res[g, 0]

    def give_back(g):
        for made in xb_copies[g]:
            made.wait_recv()
        for n in range(0, width, tile):
            rows_in = back[g, :, :, n : n + tile].reshape(n_rows, tile)
            ret_out[g * gs : (g + 1) * gs, :, n : n + tile] = (
                mm(rev, rows_in).astype(BF16).reshape(gs, blk, tile)
            )
        for p in range(g * gs, min((g + 1) * gs, nz - 1)):
            zb_copies.append(
                send(
                    ret_out.at[p],
                    ret_in.at[p],
                    zb_s.at[p],
                    zb_r.at[p],
                    at((z + nz - offset(p)) % nz, c, x),
                )
            )

    spread(0)

    for made in a_copies:
        made.wait_recv()
    lanes = [pl.ds(n, 128) for n in range(0, dv, 128)]
    top = jnp.full((1, 128), lowest_log, F32)
    my_top = top
    memory = [jnp.zeros((hr, 128), F32) for _ in lanes]
    for step in range(n_pairs):
        w = odd * step + (1 - odd) * (n_pairs - 1 - step)
        my_top = jnp.where(w == m, top, my_top)
        for lane, part in zip(lanes, memory):
            scan_out[w, :, lane] = part.astype(BF16)
        state_top, state_total = stats[w, 0:1, :], stats[w, 1:2, :]
        new_top = jnp.maximum(state_total + top, state_top)
        keep = jnp.exp(state_total + top - new_top)
        take = jnp.exp(state_top - new_top)
        memory = [
            keep * part + take * pairs_in[w, :, lane].astype(F32)
            for lane, part in zip(lanes, memory)
        ]
        top = new_top
    top_out[...] = jnp.broadcast_to(my_top, (8, 128))
    top_copy = send(top_out, top_in, n_s.at[2], n_r.at[2], neighbour)
    mine_dir = 1 - odd
    b_copies = []
    for i in range(1, n_pairs):
        to = (m + i) % n_pairs
        b_copies.append(
            send(
                scan_out.at[to],
                far.at[mine_dir, c, m],
                b_s.at[i],
                b_r.at[i],
                at(2 * to + odd, c, x),
            )
        )
    far[mine_dir, c, m] = scan_out[m]
    z_copies += z_send(range(min(2 * gs, nz - 1), nz - 1))

    for load in loads[:3]:
        load.wait()
    for g in range(1, groups + 2):
        if g < groups:
            spread(g)
        if 0 <= g - 1 < groups:
            experts(g - 1)
        if g == 1:
            for made in b_copies:
                made.wait_recv()
            far_next = send(
                far.at[mine_dir, c], far.at[mine_dir, c], n_s.at[3], n_r.at[3], neighbour
            )
        if 0 <= g - 2 < groups:
            give_back(g - 2)
    ret_in[nz - 1] = ret_out[nz - 1]

    top_copy.wait_recv()
    copy(
        far.at[mine_dir, c], far.at[1 - mine_dir, c], n_s.at[3], n_r.at[3], neighbour
    ).wait_recv()
    halves = [(far.at[0], 2), (far.at[1], 3), (near_state, 4)]
    for ref, i in halves:
        send(ref.at[c], ref.at[c], pair_s.at[i], pair_r.at[i], partner)
    for load in first_loads[8:]:
        load.wait()
    scores = mm_t(q_ref[...], k_ref[...]) * scale
    t_par, f_par, b_par, t_near, f_near, b_near, my_top = (
        value[:, 0:1] for value in (t_par, f_par, b_par, t_near, f_near, b_near, my_top)
    )
    other_top = top_in[0:1, 0:1]
    rest_col = total - before_col
    since_start = through_col + jnp.where(first, 0.0, t_par)
    until_end = rest_col + jnp.where(first, t_par, 0.0)
    prior_log = since_start + jnp.where(later, t_near + my_top, other_top)
    later_log = until_end + jnp.where(later, other_top, t_near + my_top)
    near_log = jnp.where(later, since_start + f_near, until_end + b_near)
    pair_log = jnp.where(first, rest_col + b_par, through_col + f_par)
    row_top = jnp.maximum(
        jnp.maximum(jnp.maximum(inner_top, near_log), prior_log),
        jnp.maximum(later_log, pair_log),
    )
    weights = jnp.exp(fw_in - row_top) + jnp.exp(bw_in - row_top)
    near = (scores * weights).astype(BF16)
    for ref, i in halves:
        copy(ref.at[c], ref.at[1 - c], pair_s.at[i], pair_r.at[i], partner).wait_recv()
    queries = q_ref[...]

    def far_memory(i):
        return far[i].reshape(dqk, dv)

    head_rows = mm(near, v_ref[...]) + scale * (
        jnp.exp(prior_log - row_top) * mm(queries, far_memory(0))
        + jnp.exp(later_log - row_top) * mm(queries, far_memory(1))
        + jnp.exp(near_log - row_top) * mm(queries, near_state[...].reshape(dqk, dv))
        + jnp.exp(pair_log - row_top) * mm(queries, state_in[1 - c])
    )
    head_rows = (
        head_rows
        * lax.rsqrt(jnp.mean(head_rows * head_rows, axis=1, keepdims=True) + norm_eps)
        * head_gain_ref[...]
    )
    gated[...] = (jax.nn.sigmoid(og_ref[...].astype(F32)) * head_rows).astype(BF16)
    loads[3].wait()
    for n in range(0, width, tile):
        head_part[:, :, n : n + tile] = (
            mm(gated[...], wout[:, n : n + tile]).astype(BF16).reshape(nx, span // nx, tile)
        )
    rs_copies = []
    for i in range(1, nx):
        to = (x + i) % nx
        rs_copies.append(
            send(head_part.at[to], parts_in.at[i], rs_s.at[i], rs_r.at[i], at(z, c, to))
        )
    for made in rs_copies:
        made.wait_recv()
    for n in range(0, width, tile):
        mixed = head_part[x, :, n : n + tile].astype(F32)
        for i in range(1, nx):
            mixed = mixed + parts_in[i, :, n : n + tile].astype(F32)
        mix_ref[:, n : n + tile] = mixed.astype(BF16)

    places = iota((tokens, nz * blk), 1)
    share = jnp.where(places == place_col[0], to_col(weight_ref[0:1, :]), 0.0) + jnp.where(
        places == place_col[1], to_col(weight_ref[1:2, :]), 0.0
    )
    for made in sends:
        if all(made is not other for other in zb_copies):
            made.wait_send()
    early = nz - gs

    def part(first_place, last_place, n):
        returned = ret_in[first_place:last_place, :, n : n + tile]
        return mm_split(
            share[:, first_place * blk : last_place * blk],
            returned.reshape((last_place - first_place) * blk, tile),
        )

    if early:
        for made in zb_copies[:early]:
            made.wait_recv()
        for n in range(0, width, tile):
            partial[:, n : n + tile] = part(0, early, n)
    for made in zb_copies[early:]:
        made.wait_recv()
    for n in range(0, width, tile):
        rest = part(early, nz, n)
        if early:
            rest = rest + partial[:, n : n + tile]
        exp_ref[:, n : n + tile] = rest.astype(BF16)
    for made in zb_copies:
        made.wait_send()


def hand_over(mix_in, exp_in, mix_out, exp_out):
    mix_out[...] = mix_in[...]
    exp_out[...] = exp_in[...]


def body(
    nz,
    nx,
    queries,
    head_key_rows,
    head_value_rows,
    output_gate_logits,
    log_input_gate,
    forget_gate_logits,
    extra_log_forget,
    head_norm_gain,
    memory_output_matrix,
    expert_input_tokens,
    expert_norm_gain,
    routes,
    routed_expert_weight,
    expert_gate_matrix,
    expert_up_matrix,
    expert_down_matrix,
):
    span, dqk = queries.shape
    dv = head_value_rows.shape[1]
    tokens, width = expert_input_tokens.shape
    fe = expert_gate_matrix.shape[2]
    nr = nx * cores
    blk = nr * cap
    groups = 4 if nz % 4 == 0 else 1
    gs = nz // groups
    n_pairs = nz // 2
    hr = dqk // 2 // n_pairs
    vmem = pl.BlockSpec(memory_space=pltpu.VMEM)
    hbm = pl.BlockSpec(memory_space=pl.ANY)
    dma = pltpu.SemaphoreType.DMA
    mixer_out, expert_out = pl.pallas_call(
        functools.partial(kernel, nz, nx, groups),
        out_shape=(
            jax.ShapeDtypeStruct((span // nx, width), BF16),
            jax.ShapeDtypeStruct((tokens, width), BF16),
        ),
        in_specs=[hbm] * 16,
        out_specs=(vmem, vmem),
        scratch_shapes=[
            pltpu.VMEM((1, span), F32),
            pltpu.VMEM((1, span), F32),
            pltpu.VMEM((1, span), F32),
            pltpu.VMEM((1, dv), F32),
            pltpu.VMEM((1, width), F32),
            pltpu.VMEM((2, tokens), jnp.int32),
            pltpu.VMEM((2, tokens), F32),
            pltpu.VMEM((tokens, width), BF16),
            pltpu.VMEM((span, dqk), BF16),
            pltpu.VMEM((span, dv), BF16),
            pltpu.VMEM((span, dqk), BF16),
            pltpu.VMEM((span, dv), BF16),
            pltpu.VMEM((dv, width), BF16),
            pltpu.VMEM((width, fe), BF16),
            pltpu.VMEM((width, fe), BF16),
            pltpu.VMEM((fe, width), BF16),
            pltpu.VMEM((tokens, width), BF16),
            pltpu.VMEM((nz, blk, width), BF16),
            pltpu.VMEM((nz, blk, width), BF16),
            pltpu.VMEM((groups, nr, gs * cap, width), BF16),
            pltpu.VMEM((groups, nr, gs * cap, width), BF16),
            pltpu.VMEM((gs * blk, fe), BF16),
            pltpu.VMEM((groups, nr, gs * cap, width), BF16),
            pltpu.VMEM((groups, nr, gs * cap, width), BF16),
            pltpu.VMEM((nz, blk, width), BF16),
            pltpu.VMEM((nz, blk, width), BF16),
            pltpu.VMEM((2, dqk, dv), F32),
            pltpu.VMEM((2, dqk, dv), BF16),
            pltpu.VMEM((2, dqk, dv), BF16),
            pltpu.VMEM((8, 128), F32),
            pltpu.VMEM((8, 128), F32),
            pltpu.VMEM((2, dqk // 2, dv), F32),
            pltpu.VMEM((2, dqk // 2, dv), BF16),
            pltpu.VMEM((8, 128), F32),
            pltpu.VMEM((2, dqk // 2, dv), BF16),
            pltpu.VMEM((8, 128), F32),
            pltpu.VMEM((n_pairs, hr, dv), BF16),
            pltpu.VMEM((8, 128), F32),
            pltpu.VMEM((n_pairs, hr, dv), BF16),
            pltpu.VMEM((n_pairs, 8, 128), F32),
            pltpu.VMEM((n_pairs, hr, dv), BF16),
            pltpu.VMEM((8, 128), F32),
            pltpu.VMEM((8, 128), F32),
            pltpu.VMEM((2, 2, n_pairs, hr, dv), BF16),
            pltpu.VMEM((span, dv), BF16),
            pltpu.VMEM((nx, span // nx, width), BF16),
            pltpu.VMEM((nx, span // nx, width), BF16),
            pltpu.VMEM((tokens, width), F32),
            dma((16,)),
            dma((5,)),
            dma((5,)),
            dma((4,)),
            dma((4,)),
            dma((nz,)),
            dma((nz,)),
            dma((groups, nr)),
            dma((groups, nr)),
            dma((nz,)),
            dma((nz,)),
            dma((nz,)),
            dma((nz,)),
            dma((nz,)),
            dma((nz,)),
            dma((nx,)),
            dma((nx,)),
            dma((groups, nr)),
            dma((groups, nr)),
            dma((nz,)),
            dma((nz,)),
        ],
        compiler_params=pltpu.CompilerParams(
            collective_id=0, has_side_effects=True, vmem_limit_bytes=60 * 2**20
        ),
        name="layer_step",
    )(
        log_input_gate,
        forget_gate_logits,
        extra_log_forget,
        head_norm_gain.reshape(1, dv),
        expert_norm_gain.reshape(1, width),
        routes.T,
        routed_expert_weight.T,
        expert_input_tokens,
        head_key_rows,
        head_value_rows,
        queries,
        output_gate_logits,
        memory_output_matrix,
        expert_gate_matrix,
        expert_up_matrix,
        expert_down_matrix,
    )
    return pl.pallas_call(
        hand_over,
        out_shape=(
            jax.ShapeDtypeStruct(mixer_out.shape, BF16),
            jax.ShapeDtypeStruct(expert_out.shape, BF16),
        ),
        in_specs=[vmem] * 2,
        out_specs=(vmem,) * 2,
        compiler_params=pltpu.CompilerParams(vmem_limit_bytes=60 * 2**20),
        name="hand_over",
    )(mixer_out, expert_out)


def solution(mesh):
    nz = mesh.shape["ep"] // cores
    return jax.shard_map(
        functools.partial(body, nz, mesh.shape["tp"]),
        mesh=mesh,
        in_specs=(
            P(GRP_EP, "tp"),
            P(GRP_EP, "tp"),
            P(GRP_EP, "tp"),
            P(GRP_EP, "tp"),
            P("tp", GRP_EP),
            P("tp", GRP_EP),
            P("tp", GRP_EP),
            P("tp"),
            P("tp", None),
            P(GRP_EP_TP, None),
            P(),
            P(GRP_EP_TP, None),
            P(GRP_EP_TP, None),
            P(EP_TP, None, None),
            P(EP_TP, None, None),
            P(EP_TP, None, None),
        ),
        out_specs=(P(GRP_EP_TP, None), P(GRP_EP_TP, None)),
        check_vma=False,
    )
```

```python
import functools
import math

import jax
import jax.numpy as jnp
from jax import lax
from jax.experimental import pallas as pl
from jax.experimental.pallas import tpu as pltpu
from jax.sharding import PartitionSpec as P

MESH = pl.DeviceIdType.MESH
F32 = jnp.float32
BF16 = jnp.bfloat16

GRP_EP = ("grp", "ep")
GRP_EP_TP = ("grp", "ep", "tp")
EP_TP = ("ep", "tp")

lowest_log = -1e30
norm_eps = 1e-06
layer_eps = 1e-05
cap = 2
cores = 2


def mm(a, b):
    return lax.dot_general(a, b, (((1,), (0,)), ((), ())), preferred_element_type=F32)


def mm_t(a, b):
    return lax.dot_general(a, b, (((1,), (1,)), ((), ())), preferred_element_type=F32)


def mm_split(a, b):
    high = a.astype(BF16)
    low = (a - high.astype(F32)).astype(BF16)
    return mm(high, b) + mm(low, b)


def iota(shape, dim):
    return lax.broadcasted_iota(jnp.int32, shape, dim)


def kernel(
    nz,
    nx,
    groups,
    in_gate_hbm,
    forget_hbm,
    extra_hbm,
    head_gain_hbm,
    norm_gain_hbm,
    routes_hbm,
    weight_hbm,
    tok_hbm,
    k_hbm,
    v_hbm,
    q_hbm,
    og_hbm,
    wout_hbm,
    wg_hbm,
    wu_hbm,
    wd_hbm,
    mix_ref,
    exp_ref,
    in_gate_ref,
    forget_ref,
    extra_ref,
    head_gain_ref,
    norm_gain_ref,
    routes_ref,
    weight_ref,
    tok_ref,
    k_ref,
    v_ref,
    q_ref,
    og_ref,
    wout,
    wg,
    wu,
    wd,
    normed,
    out1,
    in1,
    out2,
    in2,
    hidden,
    res,
    back,
    ret_out,
    ret_in,
    own_state,
    state_out,
    state_in,
    stat_out,
    stat_in,
    own_chip,
    chip_state,
    chip_stat,
    near_state,
    near_stat,
    pair_state,
    pair_stat,
    pairs_in,
    stats,
    scan_out,
    top_out,
    top_in,
    passed,
    far,
    gated,
    head_part,
    parts_in,
    partial,
    load_sem,
    pair_s,
    pair_r,
    n_s,
    n_r,
    z_s,
    z_r,
    x_s,
    x_r,
    a_s,
    a_r,
    t_s,
    t_r,
    b_s,
    b_r,
    rs_s,
    rs_r,
    xb_s,
    xb_r,
    zb_s,
    zb_r,
):
    ep = lax.axis_index("ep")
    x = lax.axis_index("tp")
    z = ep // cores
    c = ep % cores
    nr = nx * cores
    r = c * nx + x
    blk = nr * cap
    gs = nz // groups
    half = nz // 2
    tokens, width = tok_ref.shape
    span, dqk = q_ref.shape
    dv = v_ref.shape[1]
    tile = min(512, width)
    hr = dqk // 2 // (nz // 2)

    def at(z_, c_, x_):
        return {"ep": z_ * cores + c_, "tp": x_}

    def row_dev(r_):
        return at(z, r_ // nx, r_ % nx)

    offsets = [half] + [(half + k) % nz for i in range(1, half) for k in (-i, i)] + [0]
    if nz > 4:
        offsets.remove(1)
        offsets.insert(3, 1)

    def offset(p):
        return offsets[p]

    def copy(src, dst, ssem, rsem, dev):
        return pltpu.make_async_remote_copy(
            src_ref=src,
            dst_ref=dst,
            send_sem=ssem,
            recv_sem=rsem,
            device_id=dev,
            device_id_type=MESH,
        )

    first_loads = [
        pltpu.make_async_copy(src, dst, load_sem.at[4 + i])
        for i, (src, dst) in enumerate(
            (
                (tok_hbm, tok_ref),
                (routes_hbm, routes_ref),
                (norm_gain_hbm, norm_gain_ref),
                (in_gate_hbm, in_gate_ref),
                (forget_hbm, forget_ref),
                (extra_hbm, extra_ref),
                (k_hbm, k_ref),
                (v_hbm, v_ref),
                (q_hbm, q_ref),
                (og_hbm, og_ref),
                (head_gain_hbm, head_gain_ref),
                (weight_hbm, weight_ref),
            )
        )
    ]
    loads = [
        pltpu.make_async_copy(wg_hbm.at[0], wg, load_sem.at[0]),
        pltpu.make_async_copy(wu_hbm.at[0], wu, load_sem.at[1]),
        pltpu.make_async_copy(wd_hbm.at[0], wd, load_sem.at[2]),
        pltpu.make_async_copy(wout_hbm, wout, load_sem.at[3]),
    ]
    barrier = pltpu.get_barrier_semaphore()
    for i in range(1, nz):
        pl.semaphore_signal(
            barrier, inc=1, device_id=at((z + i) % nz, c, x), device_id_type=MESH
        )
    for i in range(1, nr):
        pl.semaphore_signal(barrier, inc=1, device_id=row_dev((r + i) % nr), device_id_type=MESH)

    for load in first_loads + loads:
        load.start()

    for load in first_loads[:3]:
        load.wait()
    t_f32 = tok_ref[...].astype(F32)
    centre = jnp.mean(t_f32, axis=1, keepdims=True)
    t_f32 = t_f32 - centre
    spread = jnp.mean(t_f32 * t_f32, axis=1, keepdims=True)
    normed[...] = (t_f32 * lax.rsqrt(spread + layer_eps) * norm_gain_ref[...]).astype(BF16)

    t0 = iota((tokens, tokens), 0)
    t1 = iota((tokens, tokens), 1)

    def to_col(row):
        return jnp.sum(jnp.where(t0 == t1, row, 0.0), axis=1, keepdims=True)

    e_row = [routes_ref[k : k + 1, :].astype(F32) for k in range(2)]
    e_col = [to_col(e) for e in e_row]

    def place(e, earlier):
        e = e.astype(jnp.int32)
        step = ((e >> int(math.log2(nr))) - z) & (nz - 1)
        p = sum(jnp.where(step == offset, p, 0) for p, offset in enumerate(offsets))
        return p * blk + (e & (nr - 1)) * cap + earlier.astype(jnp.int32)

    def one_if(mask):
        return jnp.where(mask, 1.0, 0.0)

    place_row, place_col = [], []
    for k in range(2):
        same = (e_col[0] == e_row[k]) | (e_col[1] == e_row[k])
        earlier = jnp.sum(one_if(same & (t0 < t1)), axis=0, keepdims=True)
        place_row.append(place(e_row[k], earlier))
        same = (e_row[0] == e_col[k]) | (e_row[1] == e_col[k])
        earlier = jnp.sum(one_if(same & (t1 < t0)), axis=1, keepdims=True)
        place_col.append(place(e_col[k], earlier))
    rows = iota((nz * blk, tokens), 0)
    pick = one_if((rows == place_row[0]) | (rows == place_row[1])).astype(BF16)
    for n in range(0, width, tile):
        out1[:, :, n : n + tile] = (
            mm(pick, normed[:, n : n + tile]).astype(BF16).reshape(nz, blk, tile)
        )

    for load in first_loads[3:8]:
        load.wait()
    forget = forget_ref[...]
    forget = jnp.minimum(forget, 0.0) - jnp.log1p(jnp.exp(-jnp.abs(forget))) + extra_ref[...]
    in_gate = in_gate_ref[...]
    ti = iota((span, span), 0)
    si = iota((span, span), 1)
    forget_col = jnp.sum(jnp.where(ti == si, forget, 0.0), axis=1, keepdims=True)
    through_row = jnp.sum(jnp.where(ti <= si, forget_col, 0.0), axis=0, keepdims=True)
    through_col = jnp.sum(jnp.where(si <= ti, forget, 0.0), axis=1, keepdims=True)
    before_row = through_row - forget
    before_col = through_col - forget_col
    total = jnp.sum(forget, axis=1, keepdims=True)
    fw_log = total - through_row + in_gate
    bw_log = before_row + in_gate
    fw_top = jnp.max(fw_log, axis=1, keepdims=True)
    bw_top = jnp.max(bw_log, axis=1, keepdims=True)
    keys_t = jnp.transpose(k_ref[...].astype(F32))
    values = v_ref[...]
    own_state[0] = mm_split(keys_t * jnp.exp(fw_log - fw_top), values)
    own_state[1] = mm_split(keys_t * jnp.exp(bw_log - bw_top), values)
    state_out[...] = own_state[...].astype(BF16)
    stat_out[0:1, :] = jnp.broadcast_to(fw_top, (1, 128))
    stat_out[1:2, :] = jnp.broadcast_to(bw_top, (1, 128))
    stat_out[2:3, :] = jnp.broadcast_to(total, (1, 128))
    stat_out[3:8, :] = jnp.zeros((5, 128), F32)
    pl.semaphore_wait(barrier, nz - 1 + nr - 1)

    sends = []

    def send(*args):
        made = copy(*args)
        made.start()
        sends.append(made)
        return made

    def z_send(places):
        return [
            send(
                out1.at[p],
                in1.at[p],
                z_s.at[p],
                z_r.at[p],
                at((z + offset(p)) % nz, c, x),
            )
            for p in places
        ]


    partner = at(z, 1 - c, x)
    pair_copies = [
        send(state_out, state_in, pair_s.at[0], pair_r.at[0], partner),
        send(stat_out, stat_in, pair_s.at[1], pair_r.at[1], partner),
    ]

    z_copies = z_send(range(1))
    in1[nz - 1] = out1[nz - 1]

    scale = dqk**-0.5
    fw_in = jnp.where(ti >= si, through_col - through_row + in_gate, -jnp.inf)
    bw_in = jnp.where(ti <= si, before_row - before_col + in_gate, -jnp.inf)
    inner_top = jnp.maximum(
        jnp.max(fw_in, axis=1, keepdims=True), jnp.max(bw_in, axis=1, keepdims=True)
    )

    for made in pair_copies:
        made.wait_recv()
    first = c == 0

    def row(ref, i):
        return ref[i : i + 1, :]

    f_own, b_own, t_own = (row(stat_out, i) for i in range(3))
    f_par, b_par, t_par = (row(stat_in, i) for i in range(3))
    f_own_log = f_own + jnp.where(first, t_par, 0.0)
    f_par_log = f_par + jnp.where(first, 0.0, t_own)
    b_own_log = b_own + jnp.where(first, 0.0, t_par)
    b_par_log = b_par + jnp.where(first, t_own, 0.0)
    f_chip = jnp.maximum(f_own_log, f_par_log)
    b_chip = jnp.maximum(b_own_log, b_par_log)
    mine = pl.ds(pl.multiple_of(c * (dqk // 2), dqk // 2), dqk // 2)
    for i, (own_log, par_log, top) in enumerate(
        ((f_own_log, f_par_log, f_chip), (b_own_log, b_par_log, b_chip))
    ):
        joined = (
            jnp.exp(own_log - top)[:, 0:1] * own_state[i, mine, :]
            + jnp.exp(par_log - top)[:, 0:1] * state_in[i, mine, :].astype(F32)
        )
        own_chip[i] = joined
        chip_state[i] = joined.astype(BF16)
    t_chip = t_own + t_par
    chip_stat[0:1, :] = f_chip
    chip_stat[1:2, :] = b_chip
    chip_stat[2:3, :] = t_chip
    chip_stat[3:8, :] = jnp.zeros((5, 128), F32)

    odd = z % 2
    later = odd == 1
    m = z // 2
    neighbour = at(z + 1 - 2 * odd, c, x)
    n_pairs = nz // 2
    next_copies = [
        send(chip_stat, near_stat, n_s.at[0], n_r.at[0], neighbour),
        send(chip_state.at[odd], near_state.at[c], n_s.at[1], n_r.at[1], neighbour),
    ]
    z_copies += z_send(range(1, min(gs, nz - 1)))
    for made in next_copies:
        made.wait_recv()
    f_near, b_near, t_near = (row(near_stat, i) for i in range(3))
    own_log = jnp.where(later, f_chip, b_chip)
    near_log = jnp.where(later, f_near, b_near) + t_chip
    pair_top = jnp.maximum(own_log, near_log)
    joined = (
        jnp.exp(own_log - pair_top)[:, 0:1] * own_chip[1 - odd]
        + jnp.exp(near_log - pair_top)[:, 0:1] * near_state[c].astype(F32)
    )
    pair_state[...] = joined.astype(BF16).reshape(n_pairs, hr, dv)
    pair_stat[0:1, :] = pair_top
    pair_stat[1:2, :] = t_chip + t_near
    pair_stat[2:8, :] = jnp.zeros((6, 128), F32)
    a_copies = []
    for i in range(1, n_pairs):
        to = (m + i) % n_pairs
        dev = at(2 * to + odd, c, x)
        a_copies.append(send(pair_stat, stats.at[m], t_s.at[i], t_r.at[i], dev))
        a_copies.append(send(pair_state.at[to], pairs_in.at[m], a_s.at[i], a_r.at[i], dev))
    z_copies += z_send(range(min(gs, nz - 1), min(2 * gs, nz - 1)))
    pairs_in[m] = pair_state[m]
    stats[m] = pair_stat[...]

    ga, gb = iota((gs * blk, gs * blk), 0), iota((gs * blk, gs * blk), 1)
    lc, lg, lr = (int(math.log2(n)) for n in (cap, gs, nr))
    to_row = ga >> (lc + lg)
    to_mem = (ga >> lc) & (gs - 1)
    fwd = one_if(gb == to_mem * blk + to_row * cap + (ga & (cap - 1))).astype(BF16)
    from_mem = ga >> (lc + lr)
    from_row = (ga >> lc) & (nr - 1)
    rev = one_if(gb == from_row * (gs * cap) + from_mem * cap + (ga & (cap - 1))).astype(BF16)

    x_copies, xb_copies, zb_copies = [], [], []
    n_rows = gs * blk
    fe = wg.shape[1]
    ft = min(256, fe)

    def spread(g):
        for p in range(g * gs, min((g + 1) * gs, nz - 1)):
            z_copies[p].wait_recv()
        for n in range(0, width, tile):
            rows_in = in1[g * gs : (g + 1) * gs, :, n : n + tile].reshape(n_rows, tile)
            out2[g, :, :, n : n + tile] = (
                mm(fwd, rows_in).astype(BF16).reshape(nr, gs * cap, tile)
            )
        made = []
        for i in range(1, nr):
            to = (r + i) % nr
            made.append(
                send(out2.at[g, to], in2.at[g, i], x_s.at[g, i], x_r.at[g, i], row_dev(to))
            )
        x_copies.append(made)
        in2[g, 0] = out2[g, r]

    def experts(g):
        for made in x_copies[g]:
            made.wait_recv()
        for n in range(0, fe, ft):
            arrived = in2[g].reshape(n_rows, width)
            gate_part = mm(arrived, wg[:, n : n + ft])
            up_part = mm(arrived, wu[:, n : n + ft])
            hidden[:, n : n + ft] = (gate_part * jax.nn.sigmoid(gate_part) * up_part).astype(BF16)
        for n in range(0, width, tile):
            res[g, :, :, n : n + tile] = (
                mm(hidden[...], wd[:, n : n + tile]).astype(BF16).reshape(nr, gs * cap, tile)
            )
        made = []
        for i in range(1, nr):
            to = (r + nr - i) % nr
            made.append(
                send(res.at[g, i], back.at[g, r], xb_s.at[g, i], xb_r.at[g, i], row_dev(to))
            )
        xb_copies.append(made)
        back[g, r] = res[g, 0]

    def give_back(g):
        for made in xb_copies[g]:
            made.wait_recv()
        for n in range(0, width, tile):
            rows_in = back[g, :, :, n : n + tile].reshape(n_rows, tile)
            ret_out[g * gs : (g + 1) * gs, :, n : n + tile] = (
                mm(rev, rows_in).astype(BF16).reshape(gs, blk, tile)
            )
        for p in range(g * gs, min((g + 1) * gs, nz - 1)):
            zb_copies.append(
                send(
                    ret_out.at[p],
                    ret_in.at[p],
                    zb_s.at[p],
                    zb_r.at[p],
                    at((z + nz - offset(p)) % nz, c, x),
                )
            )

    spread(0)

    for made in a_copies:
        made.wait_recv()
    lanes = [pl.ds(n, 128) for n in range(0, dv, 128)]
    top = jnp.full((1, 128), lowest_log, F32)
    my_top = top
    memory = [jnp.zeros((hr, 128), F32) for _ in lanes]
    for step in range(n_pairs):
        w = odd * step + (1 - odd) * (n_pairs - 1 - step)
        my_top = jnp.where(w == m, top, my_top)
        for lane, part in zip(lanes, memory):
            scan_out[w, :, lane] = part.astype(BF16)
        state_top, state_total = stats[w, 0:1, :], stats[w, 1:2, :]
        new_top = jnp.maximum(state_total + top, state_top)
        keep = jnp.exp(state_total + top - new_top)
        take = jnp.exp(state_top - new_top)
        memory = [
            keep * part + take * pairs_in[w, :, lane].astype(F32)
            for lane, part in zip(lanes, memory)
        ]
        top = new_top
    other = at((z + nz + 2 * odd - 1) % nz, c, x)
    pass_top = jnp.maximum(my_top + pair_stat[1:2, :], pair_top)
    top_out[...] = jnp.broadcast_to(pass_top, (8, 128))
    top_copy = send(top_out, top_in, n_s.at[2], n_r.at[2], other)
    mine_dir = 1 - odd
    b_copies = []
    for i in range(1, n_pairs):
        to = (m + i) % n_pairs
        b_copies.append(
            send(
                scan_out.at[to],
                far.at[mine_dir, c, m],
                b_s.at[i],
                b_r.at[i],
                at(2 * to + odd, c, x),
            )
        )
    far[mine_dir, c, m] = scan_out[m]
    z_copies += z_send(range(min(2 * gs, nz - 1), nz - 1))

    for load in loads[:3]:
        load.wait()
    experts(0)
    spread(1)
    experts(1)
    for made in b_copies:
        made.wait_recv()
    passed[...] = (
        jnp.exp(my_top + pair_stat[1:2, :] - pass_top)[:, 0:1]
        * far[mine_dir, c].reshape(dqk // 2, dv).astype(F32)
        + jnp.exp(pair_top - pass_top)[:, 0:1]
        * pair_state[...].reshape(dqk // 2, dv).astype(F32)
    ).astype(BF16).reshape(n_pairs, hr, dv)
    send(passed, far.at[mine_dir, c], n_s.at[3], n_r.at[3], other)
    spread(2)
    give_back(0)
    experts(2)
    spread(3)
    give_back(1)
    top_copy.wait_recv()
    copy(passed, far.at[1 - mine_dir, c], n_s.at[3], n_r.at[3], other).wait_recv()
    halves = [(far.at[0], 2), (far.at[1], 3), (near_state, 4)]
    for ref, i in halves:
        send(ref.at[c], ref.at[c], pair_s.at[i], pair_r.at[i], partner)
    experts(3)
    for load in first_loads[8:]:
        load.wait()
    scores = mm_t(q_ref[...], k_ref[...]) * scale
    t_par, f_par, b_par, t_near, f_near, b_near, my_top = (
        value[:, 0:1] for value in (t_par, f_par, b_par, t_near, f_near, b_near, my_top)
    )
    at_end = (z == 0) | (z == nz - 1)
    other_top = jnp.where(at_end, lowest_log, top_in[0:1, 0:1])
    rest_col = total - before_col
    since_start = through_col + jnp.where(first, 0.0, t_par)
    until_end = rest_col + jnp.where(first, t_par, 0.0)
    prior_log = since_start + jnp.where(later, t_near + my_top, other_top)
    later_log = until_end + jnp.where(later, other_top, t_near + my_top)
    near_log = jnp.where(later, since_start + f_near, until_end + b_near)
    pair_log = jnp.where(first, rest_col + b_par, through_col + f_par)
    row_top = jnp.maximum(
        jnp.maximum(jnp.maximum(inner_top, near_log), prior_log),
        jnp.maximum(later_log, pair_log),
    )
    weights = jnp.exp(fw_in - row_top) + jnp.exp(bw_in - row_top)
    near = (scores * weights).astype(BF16)
    for ref, i in halves:
        copy(ref.at[c], ref.at[1 - c], pair_s.at[i], pair_r.at[i], partner).wait_recv()
    queries = q_ref[...]

    def far_memory(i):
        return far[i].reshape(dqk, dv)

    head_rows = mm(near, v_ref[...]) + scale * (
        jnp.exp(prior_log - row_top) * mm(queries, far_memory(0))
        + jnp.exp(later_log - row_top) * mm(queries, far_memory(1))
        + jnp.exp(near_log - row_top) * mm(queries, near_state[...].reshape(dqk, dv))
        + jnp.exp(pair_log - row_top) * mm(queries, state_in[1 - c])
    )
    head_rows = (
        head_rows
        * lax.rsqrt(jnp.mean(head_rows * head_rows, axis=1, keepdims=True) + norm_eps)
        * head_gain_ref[...]
    )
    gated[...] = (jax.nn.sigmoid(og_ref[...].astype(F32)) * head_rows).astype(BF16)
    loads[3].wait()
    for n in range(0, width, tile):
        head_part[:, :, n : n + tile] = (
            mm(gated[...], wout[:, n : n + tile]).astype(BF16).reshape(nx, span // nx, tile)
        )
    rs_copies = []
    for i in range(1, nx):
        to = (x + i) % nx
        rs_copies.append(
            send(head_part.at[to], parts_in.at[i], rs_s.at[i], rs_r.at[i], at(z, c, to))
        )
    give_back(2)
    give_back(3)
    ret_in[nz - 1] = ret_out[nz - 1]

    for made in rs_copies:
        made.wait_recv()
    for n in range(0, width, tile):
        mixed = head_part[x, :, n : n + tile].astype(F32)
        for i in range(1, nx):
            mixed = mixed + parts_in[i, :, n : n + tile].astype(F32)
        mix_ref[:, n : n + tile] = mixed.astype(BF16)

    places = iota((tokens, nz * blk), 1)
    share = jnp.where(places == place_col[0], to_col(weight_ref[0:1, :]), 0.0) + jnp.where(
        places == place_col[1], to_col(weight_ref[1:2, :]), 0.0
    )
    for made in sends:
        if all(made is not other for other in zb_copies):
            made.wait_send()
    early = nz - gs

    def part(first_place, last_place, n):
        returned = ret_in[first_place:last_place, :, n : n + tile]
        return mm_split(
            share[:, first_place * blk : last_place * blk],
            returned.reshape((last_place - first_place) * blk, tile),
        )

    if early:
        for made in zb_copies[:early]:
            made.wait_recv()
        for n in range(0, width, tile):
            partial[:, n : n + tile] = part(0, early, n)
    for made in zb_copies[early:]:
        made.wait_recv()
    for n in range(0, width, tile):
        rest = part(early, nz, n)
        if early:
            rest = rest + partial[:, n : n + tile]
        exp_ref[:, n : n + tile] = rest.astype(BF16)
    for made in zb_copies:
        made.wait_send()


def hand_over(mix_in, exp_in, mix_out, exp_out):
    mix_out[...] = mix_in[...]
    exp_out[...] = exp_in[...]


def body(
    nz,
    nx,
    queries,
    head_key_rows,
    head_value_rows,
    output_gate_logits,
    log_input_gate,
    forget_gate_logits,
    extra_log_forget,
    head_norm_gain,
    memory_output_matrix,
    expert_input_tokens,
    expert_norm_gain,
    routes,
    routed_expert_weight,
    expert_gate_matrix,
    expert_up_matrix,
    expert_down_matrix,
):
    span, dqk = queries.shape
    dv = head_value_rows.shape[1]
    tokens, width = expert_input_tokens.shape
    fe = expert_gate_matrix.shape[2]
    nr = nx * cores
    blk = nr * cap
    groups = 4 if nz % 4 == 0 else 1
    gs = nz // groups
    n_pairs = nz // 2
    hr = dqk // 2 // n_pairs
    vmem = pl.BlockSpec(memory_space=pltpu.VMEM)
    hbm = pl.BlockSpec(memory_space=pl.ANY)
    dma = pltpu.SemaphoreType.DMA
    mixer_out, expert_out = pl.pallas_call(
        functools.partial(kernel, nz, nx, groups),
        out_shape=(
            jax.ShapeDtypeStruct((span // nx, width), BF16),
            jax.ShapeDtypeStruct((tokens, width), BF16),
        ),
        in_specs=[hbm] * 16,
        out_specs=(vmem, vmem),
        scratch_shapes=[
            pltpu.VMEM((1, span), F32),
            pltpu.VMEM((1, span), F32),
            pltpu.VMEM((1, span), F32),
            pltpu.VMEM((1, dv), F32),
            pltpu.VMEM((1, width), F32),
            pltpu.VMEM((2, tokens), jnp.int32),
            pltpu.VMEM((2, tokens), F32),
            pltpu.VMEM((tokens, width), BF16),
            pltpu.VMEM((span, dqk), BF16),
            pltpu.VMEM((span, dv), BF16),
            pltpu.VMEM((span, dqk), BF16),
            pltpu.VMEM((span, dv), BF16),
            pltpu.VMEM((dv, width), BF16),
            pltpu.VMEM((width, fe), BF16),
            pltpu.VMEM((width, fe), BF16),
            pltpu.VMEM((fe, width), BF16),
            pltpu.VMEM((tokens, width), BF16),
            pltpu.VMEM((nz, blk, width), BF16),
            pltpu.VMEM((nz, blk, width), BF16),
            pltpu.VMEM((groups, nr, gs * cap, width), BF16),
            pltpu.VMEM((groups, nr, gs * cap, width), BF16),
            pltpu.VMEM((gs * blk, fe), BF16),
            pltpu.VMEM((groups, nr, gs * cap, width), BF16),
            pltpu.VMEM((groups, nr, gs * cap, width), BF16),
            pltpu.VMEM((nz, blk, width), BF16),
            pltpu.VMEM((nz, blk, width), BF16),
            pltpu.VMEM((2, dqk, dv), F32),
            pltpu.VMEM((2, dqk, dv), BF16),
            pltpu.VMEM((2, dqk, dv), BF16),
            pltpu.VMEM((8, 128), F32),
            pltpu.VMEM((8, 128), F32),
            pltpu.VMEM((2, dqk // 2, dv), F32),
            pltpu.VMEM((2, dqk // 2, dv), BF16),
            pltpu.VMEM((8, 128), F32),
            pltpu.VMEM((2, dqk // 2, dv), BF16),
            pltpu.VMEM((8, 128), F32),
            pltpu.VMEM((n_pairs, hr, dv), BF16),
            pltpu.VMEM((8, 128), F32),
            pltpu.VMEM((n_pairs, hr, dv), BF16),
            pltpu.VMEM((n_pairs, 8, 128), F32),
            pltpu.VMEM((n_pairs, hr, dv), BF16),
            pltpu.VMEM((8, 128), F32),
            pltpu.VMEM((8, 128), F32),
            pltpu.VMEM((n_pairs, hr, dv), BF16),
            pltpu.VMEM((2, 2, n_pairs, hr, dv), BF16),
            pltpu.VMEM((span, dv), BF16),
            pltpu.VMEM((nx, span // nx, width), BF16),
            pltpu.VMEM((nx, span // nx, width), BF16),
            pltpu.VMEM((tokens, width), F32),
            dma((16,)),
            dma((5,)),
            dma((5,)),
            dma((4,)),
            dma((4,)),
            dma((nz,)),
            dma((nz,)),
            dma((groups, nr)),
            dma((groups, nr)),
            dma((nz,)),
            dma((nz,)),
            dma((nz,)),
            dma((nz,)),
            dma((nz,)),
            dma((nz,)),
            dma((nx,)),
            dma((nx,)),
            dma((groups, nr)),
            dma((groups, nr)),
            dma((nz,)),
            dma((nz,)),
        ],
        compiler_params=pltpu.CompilerParams(
            collective_id=0, has_side_effects=True, vmem_limit_bytes=60 * 2**20
        ),
        name="layer_step",
    )(
        log_input_gate,
        forget_gate_logits,
        extra_log_forget,
        head_norm_gain.reshape(1, dv),
        expert_norm_gain.reshape(1, width),
        routes.T,
        routed_expert_weight.T,
        expert_input_tokens,
        head_key_rows,
        head_value_rows,
        queries,
        output_gate_logits,
        memory_output_matrix,
        expert_gate_matrix,
        expert_up_matrix,
        expert_down_matrix,
    )
    return pl.pallas_call(
        hand_over,
        out_shape=(
            jax.ShapeDtypeStruct(mixer_out.shape, BF16),
            jax.ShapeDtypeStruct(expert_out.shape, BF16),
        ),
        in_specs=[vmem] * 2,
        out_specs=(vmem,) * 2,
        compiler_params=pltpu.CompilerParams(vmem_limit_bytes=60 * 2**20),
        name="hand_over",
    )(mixer_out, expert_out)


def solution(mesh):
    nz = mesh.shape["ep"] // cores
    return jax.shard_map(
        functools.partial(body, nz, mesh.shape["tp"]),
        mesh=mesh,
        in_specs=(
            P(GRP_EP, "tp"),
            P(GRP_EP, "tp"),
            P(GRP_EP, "tp"),
            P(GRP_EP, "tp"),
            P("tp", GRP_EP),
            P("tp", GRP_EP),
            P("tp", GRP_EP),
            P("tp"),
            P("tp", None),
            P(GRP_EP_TP, None),
            P(),
            P(GRP_EP_TP, None),
            P(GRP_EP_TP, None),
            P(EP_TP, None, None),
            P(EP_TP, None, None),
            P(EP_TP, None, None),
        ),
        out_specs=(P(GRP_EP_TP, None), P(GRP_EP_TP, None)),
        check_vma=False,
    )
```

```python
import functools
import math

import jax
import jax.numpy as jnp
from jax import lax
from jax.experimental import pallas as pl
from jax.experimental.pallas import tpu as pltpu
from jax.sharding import PartitionSpec as P

MESH = pl.DeviceIdType.MESH
F32 = jnp.float32
BF16 = jnp.bfloat16

GRP_EP = ("grp", "ep")
GRP_EP_TP = ("grp", "ep", "tp")
EP_TP = ("ep", "tp")

lowest_log = -1e30
norm_eps = 1e-06
layer_eps = 1e-05
cap = 2
cores = 2


def mm(a, b):
    return lax.dot_general(a, b, (((1,), (0,)), ((), ())), preferred_element_type=F32)


def mm_t(a, b):
    return lax.dot_general(a, b, (((1,), (1,)), ((), ())), preferred_element_type=F32)


def mm_split(a, b):
    high = a.astype(BF16)
    low = (a - high.astype(F32)).astype(BF16)
    return mm(high, b) + mm(low, b)


def iota(shape, dim):
    return lax.broadcasted_iota(jnp.int32, shape, dim)


def kernel(
    nz,
    nx,
    groups,
    in_gate_hbm,
    forget_hbm,
    extra_hbm,
    head_gain_hbm,
    norm_gain_hbm,
    routes_hbm,
    weight_hbm,
    tok_hbm,
    k_hbm,
    v_hbm,
    q_hbm,
    og_hbm,
    wout_hbm,
    wg_hbm,
    wu_hbm,
    wd_hbm,
    mix_ref,
    exp_ref,
    in_gate_ref,
    forget_ref,
    extra_ref,
    head_gain_ref,
    norm_gain_ref,
    routes_ref,
    weight_ref,
    tok_ref,
    k_ref,
    v_ref,
    q_ref,
    og_ref,
    wout,
    wg,
    wu,
    wd,
    normed,
    out1,
    in1,
    out2,
    in2,
    hidden,
    res,
    back,
    ret_out,
    ret_in,
    own_state,
    state_out,
    state_in,
    stat_out,
    stat_in,
    own_chip,
    chip_state,
    chip_stat,
    near_state,
    near_stat,
    pair_state,
    pair_stat,
    pairs_in,
    stats,
    scan_out,
    top_out,
    top_in,
    passed,
    far,
    gated,
    head_part,
    parts_in,
    partial,
    ready,
    load_sem,
    pair_s,
    pair_r,
    n_s,
    n_r,
    z_s,
    z_r,
    x_s,
    x_r,
    a_s,
    a_r,
    t_s,
    t_r,
    b_s,
    b_r,
    rs_s,
    rs_r,
    xb_s,
    xb_r,
    zb_s,
    zb_r,
):
    ep = lax.axis_index("ep")
    x = lax.axis_index("tp")
    z = ep // cores
    c = ep % cores
    nr = nx * cores
    r = c * nx + x
    blk = nr * cap
    gs = nz // groups
    half = nz // 2
    tokens, width = tok_ref.shape
    span, dqk = q_ref.shape
    dv = v_ref.shape[1]
    tile = min(512, width)
    hr = dqk // 2 // (nz // 2)

    def at(z_, c_, x_):
        return {"ep": z_ * cores + c_, "tp": x_}

    def row_dev(r_):
        return at(z, r_ // nx, r_ % nx)

    reach = nz // 4
    rest = [half, 1] + [(half + k) % nz for i in range(1, half) for k in (-i, i)]
    offsets = [reach, nz - reach]
    offsets += [i for n, i in enumerate(rest) if i not in offsets + rest[:n]] + [0]
    cuts = [0, 2, max(2, gs), max(2, 2 * gs), nz - 1]

    def offset(p):
        return offsets[p]

    def copy(src, dst, ssem, rsem, dev):
        return pltpu.make_async_remote_copy(
            src_ref=src,
            dst_ref=dst,
            send_sem=ssem,
            recv_sem=rsem,
            device_id=dev,
            device_id_type=MESH,
        )

    first_loads = [
        pltpu.make_async_copy(src, dst, load_sem.at[4 + i])
        for i, (src, dst) in enumerate(
            (
                (tok_hbm, tok_ref),
                (routes_hbm, routes_ref),
                (norm_gain_hbm, norm_gain_ref),
                (in_gate_hbm, in_gate_ref),
                (forget_hbm, forget_ref),
                (extra_hbm, extra_ref),
                (k_hbm, k_ref),
                (v_hbm, v_ref),
                (q_hbm, q_ref),
                (og_hbm, og_ref),
                (head_gain_hbm, head_gain_ref),
                (weight_hbm, weight_ref),
            )
        )
    ]
    loads = [
        pltpu.make_async_copy(wg_hbm.at[0], wg, load_sem.at[0]),
        pltpu.make_async_copy(wu_hbm.at[0], wu, load_sem.at[1]),
        pltpu.make_async_copy(wd_hbm.at[0], wd, load_sem.at[2]),
        pltpu.make_async_copy(wout_hbm, wout, load_sem.at[3]),
    ]
    barrier = pltpu.get_barrier_semaphore()
    close = [i for i in range(1, nz) if min(i, nz - i) <= reach]
    for i in close:
        pl.semaphore_signal(
            barrier, inc=1, device_id=at((z + i) % nz, c, x), device_id_type=MESH
        )
    for i in range(1, nr):
        pl.semaphore_signal(barrier, inc=1, device_id=row_dev((r + i) % nr), device_id_type=MESH)

    for load in first_loads + loads:
        load.start()

    for load in first_loads[:3]:
        load.wait()
    t_f32 = tok_ref[...].astype(F32)
    centre = jnp.mean(t_f32, axis=1, keepdims=True)
    t_f32 = t_f32 - centre
    spread = jnp.mean(t_f32 * t_f32, axis=1, keepdims=True)
    normed[...] = (t_f32 * lax.rsqrt(spread + layer_eps) * norm_gain_ref[...]).astype(BF16)

    t0 = iota((tokens, tokens), 0)
    t1 = iota((tokens, tokens), 1)

    def to_col(row):
        return jnp.sum(jnp.where(t0 == t1, row, 0.0), axis=1, keepdims=True)

    e_row = [routes_ref[k : k + 1, :].astype(F32) for k in range(2)]
    e_col = [to_col(e) for e in e_row]

    def place(e, earlier):
        e = e.astype(jnp.int32)
        step = ((e >> int(math.log2(nr))) - z) & (nz - 1)
        p = sum(jnp.where(step == offset, p, 0) for p, offset in enumerate(offsets))
        return p * blk + (e & (nr - 1)) * cap + earlier.astype(jnp.int32)

    def one_if(mask):
        return jnp.where(mask, 1.0, 0.0)

    place_row, place_col = [], []
    for k in range(2):
        same = (e_col[0] == e_row[k]) | (e_col[1] == e_row[k])
        earlier = jnp.sum(one_if(same & (t0 < t1)), axis=0, keepdims=True)
        place_row.append(place(e_row[k], earlier))
        same = (e_row[0] == e_col[k]) | (e_row[1] == e_col[k])
        earlier = jnp.sum(one_if(same & (t1 < t0)), axis=1, keepdims=True)
        place_col.append(place(e_col[k], earlier))
    rows = iota((nz * blk, tokens), 0)
    pick = one_if((rows == place_row[0]) | (rows == place_row[1])).astype(BF16)
    for n in range(0, width, tile):
        out1[:, :, n : n + tile] = (
            mm(pick, normed[:, n : n + tile]).astype(BF16).reshape(nz, blk, tile)
        )

    for load in first_loads[3:8]:
        load.wait()
    forget = forget_ref[...]
    forget = jnp.minimum(forget, 0.0) - jnp.log1p(jnp.exp(-jnp.abs(forget))) + extra_ref[...]
    in_gate = in_gate_ref[...]
    ti = iota((span, span), 0)
    si = iota((span, span), 1)
    forget_col = jnp.sum(jnp.where(ti == si, forget, 0.0), axis=1, keepdims=True)
    through_row = jnp.sum(jnp.where(ti <= si, forget_col, 0.0), axis=0, keepdims=True)
    through_col = jnp.sum(jnp.where(si <= ti, forget, 0.0), axis=1, keepdims=True)
    before_row = through_row - forget
    before_col = through_col - forget_col
    total = jnp.sum(forget, axis=1, keepdims=True)
    fw_log = total - through_row + in_gate
    bw_log = before_row + in_gate
    fw_top = jnp.max(fw_log, axis=1, keepdims=True)
    bw_top = jnp.max(bw_log, axis=1, keepdims=True)
    keys_t = jnp.transpose(k_ref[...].astype(F32))
    values = v_ref[...]
    own_state[0] = mm_split(keys_t * jnp.exp(fw_log - fw_top), values)
    own_state[1] = mm_split(keys_t * jnp.exp(bw_log - bw_top), values)
    state_out[...] = own_state[...].astype(BF16)
    stat_out[0:1, :] = jnp.broadcast_to(fw_top, (1, 128))
    stat_out[1:2, :] = jnp.broadcast_to(bw_top, (1, 128))
    stat_out[2:3, :] = jnp.broadcast_to(total, (1, 128))
    stat_out[3:8, :] = jnp.zeros((5, 128), F32)
    pl.semaphore_wait(barrier, len(close) + nr - 1)
    for to in (z + reach, z + nz - reach):
        pl.semaphore_signal(ready, inc=1, device_id=at(to % nz, c, x), device_id_type=MESH)

    sends = []

    def send(*args):
        made = copy(*args)
        made.start()
        sends.append(made)
        return made

    def z_send(places):
        return [
            send(
                out1.at[p],
                in1.at[p],
                z_s.at[p],
                z_r.at[p],
                at((z + offset(p)) % nz, c, x),
            )
            for p in places
        ]


    partner = at(z, 1 - c, x)
    pair_copies = [
        send(state_out, state_in, pair_s.at[0], pair_r.at[0], partner),
        send(stat_out, stat_in, pair_s.at[1], pair_r.at[1], partner),
    ]

    z_copies = z_send(range(cuts[0], cuts[1]))
    in1[nz - 1] = out1[nz - 1]

    scale = dqk**-0.5
    fw_in = jnp.where(ti >= si, through_col - through_row + in_gate, -jnp.inf)
    bw_in = jnp.where(ti <= si, before_row - before_col + in_gate, -jnp.inf)
    inner_top = jnp.maximum(
        jnp.max(fw_in, axis=1, keepdims=True), jnp.max(bw_in, axis=1, keepdims=True)
    )

    for made in pair_copies:
        made.wait_recv()
    first = c == 0

    def row(ref, i):
        return ref[i : i + 1, :]

    f_own, b_own, t_own = (row(stat_out, i) for i in range(3))
    f_par, b_par, t_par = (row(stat_in, i) for i in range(3))
    f_own_log = f_own + jnp.where(first, t_par, 0.0)
    f_par_log = f_par + jnp.where(first, 0.0, t_own)
    b_own_log = b_own + jnp.where(first, 0.0, t_par)
    b_par_log = b_par + jnp.where(first, t_own, 0.0)
    f_chip = jnp.maximum(f_own_log, f_par_log)
    b_chip = jnp.maximum(b_own_log, b_par_log)
    mine = pl.ds(pl.multiple_of(c * (dqk // 2), dqk // 2), dqk // 2)
    for i, (own_log, par_log, top) in enumerate(
        ((f_own_log, f_par_log, f_chip), (b_own_log, b_par_log, b_chip))
    ):
        joined = (
            jnp.exp(own_log - top)[:, 0:1] * own_state[i, mine, :]
            + jnp.exp(par_log - top)[:, 0:1] * state_in[i, mine, :].astype(F32)
        )
        own_chip[i] = joined
        chip_state[i] = joined.astype(BF16)
    t_chip = t_own + t_par
    chip_stat[0:1, :] = f_chip
    chip_stat[1:2, :] = b_chip
    chip_stat[2:3, :] = t_chip
    chip_stat[3:8, :] = jnp.zeros((5, 128), F32)

    odd = z % 2
    later = odd == 1
    m = z // 2
    neighbour = at(z + 1 - 2 * odd, c, x)
    n_pairs = nz // 2
    next_copies = [
        send(chip_stat, near_stat, n_s.at[0], n_r.at[0], neighbour),
        send(chip_state.at[odd], near_state.at[c], n_s.at[1], n_r.at[1], neighbour),
    ]
    pl.semaphore_wait(ready, 2)
    z_copies += z_send(range(cuts[1], cuts[2]))
    for made in next_copies:
        made.wait_recv()
    f_near, b_near, t_near = (row(near_stat, i) for i in range(3))
    own_log = jnp.where(later, f_chip, b_chip)
    near_log = jnp.where(later, f_near, b_near) + t_chip
    pair_top = jnp.maximum(own_log, near_log)
    joined = (
        jnp.exp(own_log - pair_top)[:, 0:1] * own_chip[1 - odd]
        + jnp.exp(near_log - pair_top)[:, 0:1] * near_state[c].astype(F32)
    )
    pair_state[...] = joined.astype(BF16).reshape(n_pairs, hr, dv)
    pair_stat[0:1, :] = pair_top
    pair_stat[1:2, :] = t_chip + t_near
    pair_stat[2:8, :] = jnp.zeros((6, 128), F32)
    a_copies = []
    for i in range(1, n_pairs):
        to = (m + i) % n_pairs
        dev = at(2 * to + odd, c, x)
        a_copies.append(send(pair_stat, stats.at[m], t_s.at[i], t_r.at[i], dev))
        a_copies.append(send(pair_state.at[to], pairs_in.at[m], a_s.at[i], a_r.at[i], dev))
    z_copies += z_send(range(cuts[2], cuts[3]))
    pairs_in[m] = pair_state[m]
    stats[m] = pair_stat[...]

    ga, gb = iota((gs * blk, gs * blk), 0), iota((gs * blk, gs * blk), 1)
    lc, lg, lr = (int(math.log2(n)) for n in (cap, gs, nr))
    to_row = ga >> (lc + lg)
    to_mem = (ga >> lc) & (gs - 1)
    fwd = one_if(gb == to_mem * blk + to_row * cap + (ga & (cap - 1))).astype(BF16)
    from_mem = ga >> (lc + lr)
    from_row = (ga >> lc) & (nr - 1)
    rev = one_if(gb == from_row * (gs * cap) + from_mem * cap + (ga & (cap - 1))).astype(BF16)

    x_copies, xb_copies, zb_copies = [], [], []
    n_rows = gs * blk
    fe = wg.shape[1]
    ft = min(256, fe)

    def spread(g):
        for p in range(g * gs, min((g + 1) * gs, nz - 1)):
            z_copies[p].wait_recv()
        for n in range(0, width, tile):
            rows_in = in1[g * gs : (g + 1) * gs, :, n : n + tile].reshape(n_rows, tile)
            out2[g, :, :, n : n + tile] = (
                mm(fwd, rows_in).astype(BF16).reshape(nr, gs * cap, tile)
            )
        made = []
        for i in range(1, nr):
            to = (r + i) % nr
            made.append(
                send(out2.at[g, to], in2.at[g, i], x_s.at[g, i], x_r.at[g, i], row_dev(to))
            )
        x_copies.append(made)
        in2[g, 0] = out2[g, r]

    def experts(g):
        for made in x_copies[g]:
            made.wait_recv()
        for n in range(0, fe, ft):
            arrived = in2[g].reshape(n_rows, width)
            gate_part = mm(arrived, wg[:, n : n + ft])
            up_part = mm(arrived, wu[:, n : n + ft])
            hidden[:, n : n + ft] = (gate_part * jax.nn.sigmoid(gate_part) * up_part).astype(BF16)
        for n in range(0, width, tile):
            res[g, :, :, n : n + tile] = (
                mm(hidden[...], wd[:, n : n + tile]).astype(BF16).reshape(nr, gs * cap, tile)
            )
        made = []
        for i in range(1, nr):
            to = (r + nr - i) % nr
            made.append(
                send(res.at[g, i], back.at[g, r], xb_s.at[g, i], xb_r.at[g, i], row_dev(to))
            )
        xb_copies.append(made)
        back[g, r] = res[g, 0]

    def give_back(g):
        for made in xb_copies[g]:
            made.wait_recv()
        for n in range(0, width, tile):
            rows_in = back[g, :, :, n : n + tile].reshape(n_rows, tile)
            ret_out[g * gs : (g + 1) * gs, :, n : n + tile] = (
                mm(rev, rows_in).astype(BF16).reshape(gs, blk, tile)
            )
        for p in range(g * gs, min((g + 1) * gs, nz - 1)):
            zb_copies.append(
                send(
                    ret_out.at[p],
                    ret_in.at[p],
                    zb_s.at[p],
                    zb_r.at[p],
                    at((z + nz - offset(p)) % nz, c, x),
                )
            )

    spread(0)

    for made in a_copies:
        made.wait_recv()
    lanes = [pl.ds(n, 128) for n in range(0, dv, 128)]
    top = jnp.full((1, 128), lowest_log, F32)
    my_top = top
    memory = [jnp.zeros((hr, 128), F32) for _ in lanes]
    for step in range(n_pairs):
        w = odd * step + (1 - odd) * (n_pairs - 1 - step)
        my_top = jnp.where(w == m, top, my_top)
        for lane, part in zip(lanes, memory):
            scan_out[w, :, lane] = part.astype(BF16)
        state_top, state_total = stats[w, 0:1, :], stats[w, 1:2, :]
        new_top = jnp.maximum(state_total + top, state_top)
        keep = jnp.exp(state_total + top - new_top)
        take = jnp.exp(state_top - new_top)
        memory = [
            keep * part + take * pairs_in[w, :, lane].astype(F32)
            for lane, part in zip(lanes, memory)
        ]
        top = new_top
    other = at((z + nz + 2 * odd - 1) % nz, c, x)
    pass_top = jnp.maximum(my_top + pair_stat[1:2, :], pair_top)
    top_out[...] = jnp.broadcast_to(pass_top, (8, 128))
    top_copy = send(top_out, top_in, n_s.at[2], n_r.at[2], other)
    mine_dir = 1 - odd
    b_copies = []
    for i in range(1, n_pairs):
        to = (m + i) % n_pairs
        b_copies.append(
            send(
                scan_out.at[to],
                far.at[mine_dir, c, m],
                b_s.at[i],
                b_r.at[i],
                at(2 * to + odd, c, x),
            )
        )
    far[mine_dir, c, m] = scan_out[m]
    z_copies += z_send(range(cuts[3], cuts[4]))

    for load in loads[:3]:
        load.wait()
    experts(0)
    spread(1)
    experts(1)
    for made in b_copies:
        made.wait_recv()
    passed[...] = (
        jnp.exp(my_top + pair_stat[1:2, :] - pass_top)[:, 0:1]
        * far[mine_dir, c].reshape(dqk // 2, dv).astype(F32)
        + jnp.exp(pair_top - pass_top)[:, 0:1]
        * pair_state[...].reshape(dqk // 2, dv).astype(F32)
    ).astype(BF16).reshape(n_pairs, hr, dv)
    send(passed, far.at[mine_dir, c], n_s.at[3], n_r.at[3], other)
    spread(2)
    give_back(0)
    experts(2)
    spread(3)
    give_back(1)
    top_copy.wait_recv()
    copy(passed, far.at[1 - mine_dir, c], n_s.at[3], n_r.at[3], other).wait_recv()
    halves = [(far.at[0], 2), (far.at[1], 3), (near_state, 4)]
    for ref, i in halves:
        send(ref.at[c], ref.at[c], pair_s.at[i], pair_r.at[i], partner)
    experts(3)
    for load in first_loads[8:]:
        load.wait()
    scores = mm_t(q_ref[...], k_ref[...]) * scale
    t_par, f_par, b_par, t_near, f_near, b_near, my_top = (
        value[:, 0:1] for value in (t_par, f_par, b_par, t_near, f_near, b_near, my_top)
    )
    at_end = (z == 0) | (z == nz - 1)
    other_top = jnp.where(at_end, lowest_log, top_in[0:1, 0:1])
    rest_col = total - before_col
    since_start = through_col + jnp.where(first, 0.0, t_par)
    until_end = rest_col + jnp.where(first, t_par, 0.0)
    prior_log = since_start + jnp.where(later, t_near + my_top, other_top)
    later_log = until_end + jnp.where(later, other_top, t_near + my_top)
    near_log = jnp.where(later, since_start + f_near, until_end + b_near)
    pair_log = jnp.where(first, rest_col + b_par, through_col + f_par)
    row_top = jnp.maximum(
        jnp.maximum(jnp.maximum(inner_top, near_log), prior_log),
        jnp.maximum(later_log, pair_log),
    )
    weights = jnp.exp(fw_in - row_top) + jnp.exp(bw_in - row_top)
    near = (scores * weights).astype(BF16)
    for ref, i in halves:
        copy(ref.at[c], ref.at[1 - c], pair_s.at[i], pair_r.at[i], partner).wait_recv()
    queries = q_ref[...]

    def far_memory(i):
        return far[i].reshape(dqk, dv)

    head_rows = mm(near, v_ref[...]) + scale * (
        jnp.exp(prior_log - row_top) * mm(queries, far_memory(0))
        + jnp.exp(later_log - row_top) * mm(queries, far_memory(1))
        + jnp.exp(near_log - row_top) * mm(queries, near_state[...].reshape(dqk, dv))
        + jnp.exp(pair_log - row_top) * mm(queries, state_in[1 - c])
    )
    head_rows = (
        head_rows
        * lax.rsqrt(jnp.mean(head_rows * head_rows, axis=1, keepdims=True) + norm_eps)
        * head_gain_ref[...]
    )
    gated[...] = (jax.nn.sigmoid(og_ref[...].astype(F32)) * head_rows).astype(BF16)
    loads[3].wait()
    for n in range(0, width, tile):
        head_part[:, :, n : n + tile] = (
            mm(gated[...], wout[:, n : n + tile]).astype(BF16).reshape(nx, span // nx, tile)
        )
    rs_copies = []
    for i in range(1, nx):
        to = (x + i) % nx
        rs_copies.append(
            send(head_part.at[to], parts_in.at[i], rs_s.at[i], rs_r.at[i], at(z, c, to))
        )
    give_back(2)
    give_back(3)
    ret_in[nz - 1] = ret_out[nz - 1]

    for made in rs_copies:
        made.wait_recv()
    for n in range(0, width, tile):
        mixed = head_part[x, :, n : n + tile].astype(F32)
        for i in range(1, nx):
            mixed = mixed + parts_in[i, :, n : n + tile].astype(F32)
        mix_ref[:, n : n + tile] = mixed.astype(BF16)

    places = iota((tokens, nz * blk), 1)
    share = jnp.where(places == place_col[0], to_col(weight_ref[0:1, :]), 0.0) + jnp.where(
        places == place_col[1], to_col(weight_ref[1:2, :]), 0.0
    )
    for made in sends:
        if all(made is not other for other in zb_copies):
            made.wait_send()
    early = nz - gs

    def part(first_place, last_place, n):
        returned = ret_in[first_place:last_place, :, n : n + tile]
        return mm_split(
            share[:, first_place * blk : last_place * blk],
            returned.reshape((last_place - first_place) * blk, tile),
        )

    if early:
        for made in zb_copies[:early]:
            made.wait_recv()
        for n in range(0, width, tile):
            partial[:, n : n + tile] = part(0, early, n)
    for made in zb_copies[early:]:
        made.wait_recv()
    for n in range(0, width, tile):
        rest = part(early, nz, n)
        if early:
            rest = rest + partial[:, n : n + tile]
        exp_ref[:, n : n + tile] = rest.astype(BF16)
    for made in zb_copies:
        made.wait_send()


def hand_over(mix_in, exp_in, mix_out, exp_out):
    mix_out[...] = mix_in[...]
    exp_out[...] = exp_in[...]


def body(
    nz,
    nx,
    queries,
    head_key_rows,
    head_value_rows,
    output_gate_logits,
    log_input_gate,
    forget_gate_logits,
    extra_log_forget,
    head_norm_gain,
    memory_output_matrix,
    expert_input_tokens,
    expert_norm_gain,
    routes,
    routed_expert_weight,
    expert_gate_matrix,
    expert_up_matrix,
    expert_down_matrix,
):
    span, dqk = queries.shape
    dv = head_value_rows.shape[1]
    tokens, width = expert_input_tokens.shape
    fe = expert_gate_matrix.shape[2]
    nr = nx * cores
    blk = nr * cap
    groups = 4 if nz % 4 == 0 else 1
    gs = nz // groups
    n_pairs = nz // 2
    hr = dqk // 2 // n_pairs
    vmem = pl.BlockSpec(memory_space=pltpu.VMEM)
    hbm = pl.BlockSpec(memory_space=pl.ANY)
    dma = pltpu.SemaphoreType.DMA
    mixer_out, expert_out = pl.pallas_call(
        functools.partial(kernel, nz, nx, groups),
        out_shape=(
            jax.ShapeDtypeStruct((span // nx, width), BF16),
            jax.ShapeDtypeStruct((tokens, width), BF16),
        ),
        in_specs=[hbm] * 16,
        out_specs=(vmem, vmem),
        scratch_shapes=[
            pltpu.VMEM((1, span), F32),
            pltpu.VMEM((1, span), F32),
            pltpu.VMEM((1, span), F32),
            pltpu.VMEM((1, dv), F32),
            pltpu.VMEM((1, width), F32),
            pltpu.VMEM((2, tokens), jnp.int32),
            pltpu.VMEM((2, tokens), F32),
            pltpu.VMEM((tokens, width), BF16),
            pltpu.VMEM((span, dqk), BF16),
            pltpu.VMEM((span, dv), BF16),
            pltpu.VMEM((span, dqk), BF16),
            pltpu.VMEM((span, dv), BF16),
            pltpu.VMEM((dv, width), BF16),
            pltpu.VMEM((width, fe), BF16),
            pltpu.VMEM((width, fe), BF16),
            pltpu.VMEM((fe, width), BF16),
            pltpu.VMEM((tokens, width), BF16),
            pltpu.VMEM((nz, blk, width), BF16),
            pltpu.VMEM((nz, blk, width), BF16),
            pltpu.VMEM((groups, nr, gs * cap, width), BF16),
            pltpu.VMEM((groups, nr, gs * cap, width), BF16),
            pltpu.VMEM((gs * blk, fe), BF16),
            pltpu.VMEM((groups, nr, gs * cap, width), BF16),
            pltpu.VMEM((groups, nr, gs * cap, width), BF16),
            pltpu.VMEM((nz, blk, width), BF16),
            pltpu.VMEM((nz, blk, width), BF16),
            pltpu.VMEM((2, dqk, dv), F32),
            pltpu.VMEM((2, dqk, dv), BF16),
            pltpu.VMEM((2, dqk, dv), BF16),
            pltpu.VMEM((8, 128), F32),
            pltpu.VMEM((8, 128), F32),
            pltpu.VMEM((2, dqk // 2, dv), F32),
            pltpu.VMEM((2, dqk // 2, dv), BF16),
            pltpu.VMEM((8, 128), F32),
            pltpu.VMEM((2, dqk // 2, dv), BF16),
            pltpu.VMEM((8, 128), F32),
            pltpu.VMEM((n_pairs, hr, dv), BF16),
            pltpu.VMEM((8, 128), F32),
            pltpu.VMEM((n_pairs, hr, dv), BF16),
            pltpu.VMEM((n_pairs, 8, 128), F32),
            pltpu.VMEM((n_pairs, hr, dv), BF16),
            pltpu.VMEM((8, 128), F32),
            pltpu.VMEM((8, 128), F32),
            pltpu.VMEM((n_pairs, hr, dv), BF16),
            pltpu.VMEM((2, 2, n_pairs, hr, dv), BF16),
            pltpu.VMEM((span, dv), BF16),
            pltpu.VMEM((nx, span // nx, width), BF16),
            pltpu.VMEM((nx, span // nx, width), BF16),
            pltpu.VMEM((tokens, width), F32),
            pltpu.SemaphoreType.REGULAR,
            dma((16,)),
            dma((5,)),
            dma((5,)),
            dma((4,)),
            dma((4,)),
            dma((nz,)),
            dma((nz,)),
            dma((groups, nr)),
            dma((groups, nr)),
            dma((nz,)),
            dma((nz,)),
            dma((nz,)),
            dma((nz,)),
            dma((nz,)),
            dma((nz,)),
            dma((nx,)),
            dma((nx,)),
            dma((groups, nr)),
            dma((groups, nr)),
            dma((nz,)),
            dma((nz,)),
        ],
        compiler_params=pltpu.CompilerParams(
            collective_id=0, has_side_effects=True, vmem_limit_bytes=60 * 2**20
        ),
        name="layer_step",
    )(
        log_input_gate,
        forget_gate_logits,
        extra_log_forget,
        head_norm_gain.reshape(1, dv),
        expert_norm_gain.reshape(1, width),
        routes.T,
        routed_expert_weight.T,
        expert_input_tokens,
        head_key_rows,
        head_value_rows,
        queries,
        output_gate_logits,
        memory_output_matrix,
        expert_gate_matrix,
        expert_up_matrix,
        expert_down_matrix,
    )
    return pl.pallas_call(
        hand_over,
        out_shape=(
            jax.ShapeDtypeStruct(mixer_out.shape, BF16),
            jax.ShapeDtypeStruct(expert_out.shape, BF16),
        ),
        in_specs=[vmem] * 2,
        out_specs=(vmem,) * 2,
        compiler_params=pltpu.CompilerParams(vmem_limit_bytes=60 * 2**20),
        name="hand_over",
    )(mixer_out, expert_out)


def solution(mesh):
    nz = mesh.shape["ep"] // cores
    return jax.shard_map(
        functools.partial(body, nz, mesh.shape["tp"]),
        mesh=mesh,
        in_specs=(
            P(GRP_EP, "tp"),
            P(GRP_EP, "tp"),
            P(GRP_EP, "tp"),
            P(GRP_EP, "tp"),
            P("tp", GRP_EP),
            P("tp", GRP_EP),
            P("tp", GRP_EP),
            P("tp"),
            P("tp", None),
            P(GRP_EP_TP, None),
            P(),
            P(GRP_EP_TP, None),
            P(GRP_EP_TP, None),
            P(EP_TP, None, None),
            P(EP_TP, None, None),
            P(EP_TP, None, None),
        ),
        out_specs=(P(GRP_EP_TP, None), P(GRP_EP_TP, None)),
        check_vma=False,
    )
```

```python
import functools
import math

import jax
import jax.numpy as jnp
from jax import lax
from jax.experimental import pallas as pl
from jax.experimental.pallas import tpu as pltpu
from jax.sharding import PartitionSpec as P

MESH = pl.DeviceIdType.MESH
F32 = jnp.float32
BF16 = jnp.bfloat16

GRP_EP = ("grp", "ep")
GRP_EP_TP = ("grp", "ep", "tp")
EP_TP = ("ep", "tp")

lowest_log = -1e30
norm_eps = 1e-06
layer_eps = 1e-05
cap = 2
cores = 2


def mm(a, b):
    return lax.dot_general(a, b, (((1,), (0,)), ((), ())), preferred_element_type=F32)


def mm_t(a, b):
    return lax.dot_general(a, b, (((1,), (1,)), ((), ())), preferred_element_type=F32)


def mm_split(a, b):
    high = a.astype(BF16)
    low = (a - high.astype(F32)).astype(BF16)
    return mm(high, b) + mm(low, b)


def iota(shape, dim):
    return lax.broadcasted_iota(jnp.int32, shape, dim)


def kernel(
    nz,
    nx,
    groups,
    in_gate_hbm,
    forget_hbm,
    extra_hbm,
    head_gain_hbm,
    norm_gain_hbm,
    routes_hbm,
    weight_hbm,
    tok_hbm,
    k_hbm,
    v_hbm,
    q_hbm,
    og_hbm,
    wout_hbm,
    wg_hbm,
    wu_hbm,
    wd_hbm,
    mix_hbm,
    exp_hbm,
    mix_ref,
    exp_ref,
    in_gate_ref,
    forget_ref,
    extra_ref,
    head_gain_ref,
    norm_gain_ref,
    routes_ref,
    weight_ref,
    tok_ref,
    k_ref,
    v_ref,
    q_ref,
    og_ref,
    wout,
    wg,
    wu,
    wd,
    normed,
    out1,
    in1,
    out2,
    in2,
    hidden,
    res,
    back,
    ret_out,
    ret_in,
    own_state,
    state_out,
    state_in,
    stat_out,
    stat_in,
    own_chip,
    chip_state,
    chip_stat,
    near_state,
    near_stat,
    pair_state,
    pair_stat,
    pairs_in,
    stats,
    scan_out,
    top_out,
    top_in,
    passed,
    far,
    gated,
    head_part,
    parts_in,
    partial,
    ready,
    store_sem,
    load_sem,
    pair_s,
    pair_r,
    n_s,
    n_r,
    z_s,
    z_r,
    x_s,
    x_r,
    a_s,
    a_r,
    t_s,
    t_r,
    b_s,
    b_r,
    rs_s,
    rs_r,
    xb_s,
    xb_r,
    zb_s,
    zb_r,
):
    ep = lax.axis_index("ep")
    x = lax.axis_index("tp")
    z = ep // cores
    c = ep % cores
    nr = nx * cores
    r = c * nx + x
    blk = nr * cap
    gs = nz // groups
    half = nz // 2
    tokens, width = tok_ref.shape
    span, dqk = q_ref.shape
    dv = v_ref.shape[1]
    tile = min(512, width)
    hr = dqk // 2 // (nz // 2)

    def at(z_, c_, x_):
        return {"ep": z_ * cores + c_, "tp": x_}

    def row_dev(r_):
        return at(z, r_ // nx, r_ % nx)

    reach = nz // 4
    rest = [half, 1] + [(half + k) % nz for i in range(1, half) for k in (-i, i)]
    offsets = [reach, nz - reach]
    offsets += [i for n, i in enumerate(rest) if i not in offsets + rest[:n]] + [0]
    cuts = [0, 2, max(2, gs), max(2, 2 * gs), nz - 1]

    def offset(p):
        return offsets[p]

    def copy(src, dst, ssem, rsem, dev):
        return pltpu.make_async_remote_copy(
            src_ref=src,
            dst_ref=dst,
            send_sem=ssem,
            recv_sem=rsem,
            device_id=dev,
            device_id_type=MESH,
        )

    first_loads = [
        pltpu.make_async_copy(src, dst, load_sem.at[4 + i])
        for i, (src, dst) in enumerate(
            (
                (tok_hbm, tok_ref),
                (routes_hbm, routes_ref),
                (norm_gain_hbm, norm_gain_ref),
                (in_gate_hbm, in_gate_ref),
                (forget_hbm, forget_ref),
                (extra_hbm, extra_ref),
                (k_hbm, k_ref),
                (v_hbm, v_ref),
                (q_hbm, q_ref),
                (og_hbm, og_ref),
                (head_gain_hbm, head_gain_ref),
                (weight_hbm, weight_ref),
            )
        )
    ]
    loads = [
        pltpu.make_async_copy(wg_hbm.at[0], wg, load_sem.at[0]),
        pltpu.make_async_copy(wu_hbm.at[0], wu, load_sem.at[1]),
        pltpu.make_async_copy(wd_hbm.at[0], wd, load_sem.at[2]),
        pltpu.make_async_copy(wout_hbm, wout, load_sem.at[3]),
    ]
    barrier = pltpu.get_barrier_semaphore()
    close = [i for i in range(1, nz) if min(i, nz - i) <= reach]
    for i in close:
        pl.semaphore_signal(
            barrier, inc=1, device_id=at((z + i) % nz, c, x), device_id_type=MESH
        )
    for i in range(1, nr):
        pl.semaphore_signal(barrier, inc=1, device_id=row_dev((r + i) % nr), device_id_type=MESH)

    for load in first_loads + loads:
        load.start()

    for load in first_loads[:3]:
        load.wait()
    t_f32 = tok_ref[...].astype(F32)
    centre = jnp.mean(t_f32, axis=1, keepdims=True)
    t_f32 = t_f32 - centre
    spread = jnp.mean(t_f32 * t_f32, axis=1, keepdims=True)
    normed[...] = (t_f32 * lax.rsqrt(spread + layer_eps) * norm_gain_ref[...]).astype(BF16)

    t0 = iota((tokens, tokens), 0)
    t1 = iota((tokens, tokens), 1)

    def to_col(row):
        return jnp.sum(jnp.where(t0 == t1, row, 0.0), axis=1, keepdims=True)

    e_row = [routes_ref[k : k + 1, :].astype(F32) for k in range(2)]
    e_col = [to_col(e) for e in e_row]

    def place(e, earlier):
        e = e.astype(jnp.int32)
        step = ((e >> int(math.log2(nr))) - z) & (nz - 1)
        p = sum(jnp.where(step == offset, p, 0) for p, offset in enumerate(offsets))
        return p * blk + (e & (nr - 1)) * cap + earlier.astype(jnp.int32)

    def one_if(mask):
        return jnp.where(mask, 1.0, 0.0)

    place_row, place_col = [], []
    for k in range(2):
        same = (e_col[0] == e_row[k]) | (e_col[1] == e_row[k])
        earlier = jnp.sum(one_if(same & (t0 < t1)), axis=0, keepdims=True)
        place_row.append(place(e_row[k], earlier))
        same = (e_row[0] == e_col[k]) | (e_row[1] == e_col[k])
        earlier = jnp.sum(one_if(same & (t1 < t0)), axis=1, keepdims=True)
        place_col.append(place(e_col[k], earlier))
    rows = iota((nz * blk, tokens), 0)
    pick = one_if((rows == place_row[0]) | (rows == place_row[1])).astype(BF16)
    for n in range(0, width, tile):
        out1[:, :, n : n + tile] = (
            mm(pick, normed[:, n : n + tile]).astype(BF16).reshape(nz, blk, tile)
        )

    for load in first_loads[3:8]:
        load.wait()
    forget = forget_ref[...]
    forget = jnp.minimum(forget, 0.0) - jnp.log1p(jnp.exp(-jnp.abs(forget))) + extra_ref[...]
    in_gate = in_gate_ref[...]
    ti = iota((span, span), 0)
    si = iota((span, span), 1)
    forget_col = jnp.sum(jnp.where(ti == si, forget, 0.0), axis=1, keepdims=True)
    through_row = jnp.sum(jnp.where(ti <= si, forget_col, 0.0), axis=0, keepdims=True)
    through_col = jnp.sum(jnp.where(si <= ti, forget, 0.0), axis=1, keepdims=True)
    before_row = through_row - forget
    before_col = through_col - forget_col
    total = jnp.sum(forget, axis=1, keepdims=True)
    fw_log = total - through_row + in_gate
    bw_log = before_row + in_gate
    fw_top = jnp.max(fw_log, axis=1, keepdims=True)
    bw_top = jnp.max(bw_log, axis=1, keepdims=True)
    keys_t = jnp.transpose(k_ref[...].astype(F32))
    values = v_ref[...]
    own_state[0] = mm_split(keys_t * jnp.exp(fw_log - fw_top), values)
    own_state[1] = mm_split(keys_t * jnp.exp(bw_log - bw_top), values)
    state_out[...] = own_state[...].astype(BF16)
    stat_out[0:1, :] = jnp.broadcast_to(fw_top, (1, 128))
    stat_out[1:2, :] = jnp.broadcast_to(bw_top, (1, 128))
    stat_out[2:3, :] = jnp.broadcast_to(total, (1, 128))
    stat_out[3:8, :] = jnp.zeros((5, 128), F32)
    pl.semaphore_wait(barrier, len(close) + nr - 1)
    for to in (z + reach, z + nz - reach):
        pl.semaphore_signal(ready, inc=1, device_id=at(to % nz, c, x), device_id_type=MESH)

    sends = []

    def send(*args):
        made = copy(*args)
        made.start()
        sends.append(made)
        return made

    def z_send(places):
        return [
            send(
                out1.at[p],
                in1.at[p],
                z_s.at[p],
                z_r.at[p],
                at((z + offset(p)) % nz, c, x),
            )
            for p in places
        ]


    partner = at(z, 1 - c, x)
    pair_copies = [
        send(state_out, state_in, pair_s.at[0], pair_r.at[0], partner),
        send(stat_out, stat_in, pair_s.at[1], pair_r.at[1], partner),
    ]

    z_copies = z_send(range(cuts[0], cuts[1]))
    in1[nz - 1] = out1[nz - 1]

    scale = dqk**-0.5
    fw_in = jnp.where(ti >= si, through_col - through_row + in_gate, -jnp.inf)
    bw_in = jnp.where(ti <= si, before_row - before_col + in_gate, -jnp.inf)
    inner_top = jnp.maximum(
        jnp.max(fw_in, axis=1, keepdims=True), jnp.max(bw_in, axis=1, keepdims=True)
    )

    for made in pair_copies:
        made.wait_recv()
    first = c == 0

    def row(ref, i):
        return ref[i : i + 1, :]

    f_own, b_own, t_own = (row(stat_out, i) for i in range(3))
    f_par, b_par, t_par = (row(stat_in, i) for i in range(3))
    f_own_log = f_own + jnp.where(first, t_par, 0.0)
    f_par_log = f_par + jnp.where(first, 0.0, t_own)
    b_own_log = b_own + jnp.where(first, 0.0, t_par)
    b_par_log = b_par + jnp.where(first, t_own, 0.0)
    f_chip = jnp.maximum(f_own_log, f_par_log)
    b_chip = jnp.maximum(b_own_log, b_par_log)
    mine = pl.ds(pl.multiple_of(c * (dqk // 2), dqk // 2), dqk // 2)
    for i, (own_log, par_log, top) in enumerate(
        ((f_own_log, f_par_log, f_chip), (b_own_log, b_par_log, b_chip))
    ):
        joined = (
            jnp.exp(own_log - top)[:, 0:1] * own_state[i, mine, :]
            + jnp.exp(par_log - top)[:, 0:1] * state_in[i, mine, :].astype(F32)
        )
        own_chip[i] = joined
        chip_state[i] = joined.astype(BF16)
    t_chip = t_own + t_par
    chip_stat[0:1, :] = f_chip
    chip_stat[1:2, :] = b_chip
    chip_stat[2:3, :] = t_chip
    chip_stat[3:8, :] = jnp.zeros((5, 128), F32)

    odd = z % 2
    later = odd == 1
    m = z // 2
    neighbour = at(z + 1 - 2 * odd, c, x)
    n_pairs = nz // 2
    next_copies = [
        send(chip_stat, near_stat, n_s.at[0], n_r.at[0], neighbour),
        send(chip_state.at[odd], near_state.at[c], n_s.at[1], n_r.at[1], neighbour),
    ]
    pl.semaphore_wait(ready, 2)
    z_copies += z_send(range(cuts[1], cuts[2]))
    for made in next_copies:
        made.wait_recv()
    f_near, b_near, t_near = (row(near_stat, i) for i in range(3))
    own_log = jnp.where(later, f_chip, b_chip)
    near_log = jnp.where(later, f_near, b_near) + t_chip
    pair_top = jnp.maximum(own_log, near_log)
    joined = (
        jnp.exp(own_log - pair_top)[:, 0:1] * own_chip[1 - odd]
        + jnp.exp(near_log - pair_top)[:, 0:1] * near_state[c].astype(F32)
    )
    pair_state[...] = joined.astype(BF16).reshape(n_pairs, hr, dv)
    pair_stat[0:1, :] = pair_top
    pair_stat[1:2, :] = t_chip + t_near
    pair_stat[2:8, :] = jnp.zeros((6, 128), F32)
    a_copies = []
    for i in range(1, n_pairs):
        to = (m + i) % n_pairs
        dev = at(2 * to + odd, c, x)
        a_copies.append(send(pair_stat, stats.at[m], t_s.at[i], t_r.at[i], dev))
        a_copies.append(send(pair_state.at[to], pairs_in.at[m], a_s.at[i], a_r.at[i], dev))
    z_copies += z_send(range(cuts[2], cuts[3]))
    pairs_in[m] = pair_state[m]
    stats[m] = pair_stat[...]

    ga, gb = iota((gs * blk, gs * blk), 0), iota((gs * blk, gs * blk), 1)
    lc, lg, lr = (int(math.log2(n)) for n in (cap, gs, nr))
    to_row = ga >> (lc + lg)
    to_mem = (ga >> lc) & (gs - 1)
    fwd = one_if(gb == to_mem * blk + to_row * cap + (ga & (cap - 1))).astype(BF16)
    from_mem = ga >> (lc + lr)
    from_row = (ga >> lc) & (nr - 1)
    rev = one_if(gb == from_row * (gs * cap) + from_mem * cap + (ga & (cap - 1))).astype(BF16)

    x_copies, xb_copies, zb_copies = [], [], []
    n_rows = gs * blk
    fe = wg.shape[1]
    ft = min(256, fe)

    def spread(g):
        for p in range(g * gs, min((g + 1) * gs, nz - 1)):
            z_copies[p].wait_recv()
        for n in range(0, width, tile):
            rows_in = in1[g * gs : (g + 1) * gs, :, n : n + tile].reshape(n_rows, tile)
            out2[g, :, :, n : n + tile] = (
                mm(fwd, rows_in).astype(BF16).reshape(nr, gs * cap, tile)
            )
        made = []
        for i in range(1, nr):
            to = (r + i) % nr
            made.append(
                send(out2.at[g, to], in2.at[g, i], x_s.at[g, i], x_r.at[g, i], row_dev(to))
            )
        x_copies.append(made)
        in2[g, 0] = out2[g, r]

    def experts(g):
        for made in x_copies[g]:
            made.wait_recv()
        for n in range(0, fe, ft):
            arrived = in2[g].reshape(n_rows, width)
            gate_part = mm(arrived, wg[:, n : n + ft])
            up_part = mm(arrived, wu[:, n : n + ft])
            hidden[:, n : n + ft] = (gate_part * jax.nn.sigmoid(gate_part) * up_part).astype(BF16)
        for n in range(0, width, tile):
            res[g, :, :, n : n + tile] = (
                mm(hidden[...], wd[:, n : n + tile]).astype(BF16).reshape(nr, gs * cap, tile)
            )
        made = []
        for i in range(1, nr):
            to = (r + nr - i) % nr
            made.append(
                send(res.at[g, i], back.at[g, r], xb_s.at[g, i], xb_r.at[g, i], row_dev(to))
            )
        xb_copies.append(made)
        back[g, r] = res[g, 0]

    def give_back(g):
        for made in xb_copies[g]:
            made.wait_recv()
        for n in range(0, width, tile):
            rows_in = back[g, :, :, n : n + tile].reshape(n_rows, tile)
            ret_out[g * gs : (g + 1) * gs, :, n : n + tile] = (
                mm(rev, rows_in).astype(BF16).reshape(gs, blk, tile)
            )
        for p in range(g * gs, min((g + 1) * gs, nz - 1)):
            zb_copies.append(
                send(
                    ret_out.at[p],
                    ret_in.at[p],
                    zb_s.at[p],
                    zb_r.at[p],
                    at((z + nz - offset(p)) % nz, c, x),
                )
            )

    spread(0)

    for made in a_copies:
        made.wait_recv()
    lanes = [pl.ds(n, 128) for n in range(0, dv, 128)]
    top = jnp.full((1, 128), lowest_log, F32)
    my_top = top
    memory = [jnp.zeros((hr, 128), F32) for _ in lanes]
    for step in range(n_pairs):
        w = odd * step + (1 - odd) * (n_pairs - 1 - step)
        my_top = jnp.where(w == m, top, my_top)
        for lane, part in zip(lanes, memory):
            scan_out[w, :, lane] = part.astype(BF16)
        state_top, state_total = stats[w, 0:1, :], stats[w, 1:2, :]
        new_top = jnp.maximum(state_total + top, state_top)
        keep = jnp.exp(state_total + top - new_top)
        take = jnp.exp(state_top - new_top)
        memory = [
            keep * part + take * pairs_in[w, :, lane].astype(F32)
            for lane, part in zip(lanes, memory)
        ]
        top = new_top
    other = at((z + nz + 2 * odd - 1) % nz, c, x)
    pass_top = jnp.maximum(my_top + pair_stat[1:2, :], pair_top)
    top_out[...] = jnp.broadcast_to(pass_top, (8, 128))
    top_copy = send(top_out, top_in, n_s.at[2], n_r.at[2], other)
    mine_dir = 1 - odd
    b_copies = []
    for i in range(1, n_pairs):
        to = (m + i) % n_pairs
        b_copies.append(
            send(
                scan_out.at[to],
                far.at[mine_dir, c, m],
                b_s.at[i],
                b_r.at[i],
                at(2 * to + odd, c, x),
            )
        )
    far[mine_dir, c, m] = scan_out[m]
    z_copies += z_send(range(cuts[3], cuts[4]))

    for load in loads[:3]:
        load.wait()
    experts(0)
    spread(1)
    experts(1)
    for made in b_copies:
        made.wait_recv()
    passed[...] = (
        jnp.exp(my_top + pair_stat[1:2, :] - pass_top)[:, 0:1]
        * far[mine_dir, c].reshape(dqk // 2, dv).astype(F32)
        + jnp.exp(pair_top - pass_top)[:, 0:1]
        * pair_state[...].reshape(dqk // 2, dv).astype(F32)
    ).astype(BF16).reshape(n_pairs, hr, dv)
    send(passed, far.at[mine_dir, c], n_s.at[3], n_r.at[3], other)
    spread(2)
    give_back(0)
    experts(2)
    spread(3)
    give_back(1)
    top_copy.wait_recv()
    copy(passed, far.at[1 - mine_dir, c], n_s.at[3], n_r.at[3], other).wait_recv()
    halves = [(far.at[0], 2), (far.at[1], 3), (near_state, 4)]
    for ref, i in halves:
        send(ref.at[c], ref.at[c], pair_s.at[i], pair_r.at[i], partner)
    experts(3)
    for load in first_loads[8:]:
        load.wait()
    scores = mm_t(q_ref[...], k_ref[...]) * scale
    t_par, f_par, b_par, t_near, f_near, b_near, my_top = (
        value[:, 0:1] for value in (t_par, f_par, b_par, t_near, f_near, b_near, my_top)
    )
    at_end = (z == 0) | (z == nz - 1)
    other_top = jnp.where(at_end, lowest_log, top_in[0:1, 0:1])
    rest_col = total - before_col
    since_start = through_col + jnp.where(first, 0.0, t_par)
    until_end = rest_col + jnp.where(first, t_par, 0.0)
    prior_log = since_start + jnp.where(later, t_near + my_top, other_top)
    later_log = until_end + jnp.where(later, other_top, t_near + my_top)
    near_log = jnp.where(later, since_start + f_near, until_end + b_near)
    pair_log = jnp.where(first, rest_col + b_par, through_col + f_par)
    row_top = jnp.maximum(
        jnp.maximum(jnp.maximum(inner_top, near_log), prior_log),
        jnp.maximum(later_log, pair_log),
    )
    weights = jnp.exp(fw_in - row_top) + jnp.exp(bw_in - row_top)
    near = (scores * weights).astype(BF16)
    for ref, i in halves:
        copy(ref.at[c], ref.at[1 - c], pair_s.at[i], pair_r.at[i], partner).wait_recv()
    queries = q_ref[...]

    def far_memory(i):
        return far[i].reshape(dqk, dv)

    head_rows = mm(near, v_ref[...]) + scale * (
        jnp.exp(prior_log - row_top) * mm(queries, far_memory(0))
        + jnp.exp(later_log - row_top) * mm(queries, far_memory(1))
        + jnp.exp(near_log - row_top) * mm(queries, near_state[...].reshape(dqk, dv))
        + jnp.exp(pair_log - row_top) * mm(queries, state_in[1 - c])
    )
    head_rows = (
        head_rows
        * lax.rsqrt(jnp.mean(head_rows * head_rows, axis=1, keepdims=True) + norm_eps)
        * head_gain_ref[...]
    )
    gated[...] = (jax.nn.sigmoid(og_ref[...].astype(F32)) * head_rows).astype(BF16)
    loads[3].wait()
    for n in range(0, width, tile):
        head_part[:, :, n : n + tile] = (
            mm(gated[...], wout[:, n : n + tile]).astype(BF16).reshape(nx, span // nx, tile)
        )
    rs_copies = []
    for i in range(1, nx):
        to = (x + i) % nx
        rs_copies.append(
            send(head_part.at[to], parts_in.at[i], rs_s.at[i], rs_r.at[i], at(z, c, to))
        )
    give_back(2)
    give_back(3)
    ret_in[nz - 1] = ret_out[nz - 1]

    for made in rs_copies:
        made.wait_recv()
    for n in range(0, width, tile):
        mixed = head_part[x, :, n : n + tile].astype(F32)
        for i in range(1, nx):
            mixed = mixed + parts_in[i, :, n : n + tile].astype(F32)
        mix_ref[:, n : n + tile] = mixed.astype(BF16)
    stores = [pltpu.make_async_copy(mix_ref, mix_hbm, store_sem.at[0])]
    stores[0].start()

    places = iota((tokens, nz * blk), 1)
    share = jnp.where(places == place_col[0], to_col(weight_ref[0:1, :]), 0.0) + jnp.where(
        places == place_col[1], to_col(weight_ref[1:2, :]), 0.0
    )
    for made in sends:
        if all(made is not other for other in zb_copies):
            made.wait_send()
    early = nz - gs

    def part(first_place, last_place, n):
        returned = ret_in[first_place:last_place, :, n : n + tile]
        return mm_split(
            share[:, first_place * blk : last_place * blk],
            returned.reshape((last_place - first_place) * blk, tile),
        )

    if early:
        for made in zb_copies[:early]:
            made.wait_recv()
        for n in range(0, width, tile):
            partial[:, n : n + tile] = part(0, early, n)
    for made in zb_copies[early:]:
        made.wait_recv()
    for n in range(0, width, tile):
        rest = part(early, nz, n)
        if early:
            rest = rest + partial[:, n : n + tile]
        exp_ref[:, n : n + tile] = rest.astype(BF16)
        stores.append(
            pltpu.make_async_copy(
                exp_ref.at[:, n : n + tile],
                exp_hbm.at[:, n : n + tile],
                store_sem.at[len(stores)],
            )
        )
        stores[-1].start()
    for made in zb_copies:
        made.wait_send()
    for made in stores:
        made.wait()


def hand_over(mix_in, exp_in, mix_out, exp_out, mix_ref, exp_ref, in_sem, out_sem):
    ways = ((mix_in, mix_ref, mix_out), (exp_in, exp_ref, exp_out))
    moves = []
    for i, (src, held, dst) in enumerate(ways):
        half = src.shape[0] // 2
        for k in range(2):
            part = pl.ds(k * half, half)
            n = 2 * i + k
            moves.append(
                (
                    pltpu.make_async_copy(src.at[part], held.at[part], in_sem.at[n]),
                    pltpu.make_async_copy(held.at[part], dst.at[part], out_sem.at[n]),
                )
            )
    for come, _ in moves:
        come.start()
    for come, leave in moves:
        come.wait()
        leave.start()
    for _, leave in moves:
        leave.wait()


def body(
    nz,
    nx,
    queries,
    head_key_rows,
    head_value_rows,
    output_gate_logits,
    log_input_gate,
    forget_gate_logits,
    extra_log_forget,
    head_norm_gain,
    memory_output_matrix,
    expert_input_tokens,
    expert_norm_gain,
    routes,
    routed_expert_weight,
    expert_gate_matrix,
    expert_up_matrix,
    expert_down_matrix,
):
    span, dqk = queries.shape
    dv = head_value_rows.shape[1]
    tokens, width = expert_input_tokens.shape
    fe = expert_gate_matrix.shape[2]
    nr = nx * cores
    blk = nr * cap
    groups = 4 if nz % 4 == 0 else 1
    gs = nz // groups
    n_pairs = nz // 2
    hr = dqk // 2 // n_pairs
    vmem = pl.BlockSpec(memory_space=pltpu.VMEM)
    hbm = pl.BlockSpec(memory_space=pl.ANY)
    dma = pltpu.SemaphoreType.DMA
    mixer_out, expert_out = pl.pallas_call(
        functools.partial(kernel, nz, nx, groups),
        out_shape=(
            jax.ShapeDtypeStruct((span // nx, width), BF16),
            jax.ShapeDtypeStruct((tokens, width), BF16),
        ),
        in_specs=[hbm] * 16,
        out_specs=(hbm, hbm),
        scratch_shapes=[
            pltpu.VMEM((span // nx, width), BF16),
            pltpu.VMEM((tokens, width), BF16),
            pltpu.VMEM((1, span), F32),
            pltpu.VMEM((1, span), F32),
            pltpu.VMEM((1, span), F32),
            pltpu.VMEM((1, dv), F32),
            pltpu.VMEM((1, width), F32),
            pltpu.VMEM((2, tokens), jnp.int32),
            pltpu.VMEM((2, tokens), F32),
            pltpu.VMEM((tokens, width), BF16),
            pltpu.VMEM((span, dqk), BF16),
            pltpu.VMEM((span, dv), BF16),
            pltpu.VMEM((span, dqk), BF16),
            pltpu.VMEM((span, dv), BF16),
            pltpu.VMEM((dv, width), BF16),
            pltpu.VMEM((width, fe), BF16),
            pltpu.VMEM((width, fe), BF16),
            pltpu.VMEM((fe, width), BF16),
            pltpu.VMEM((tokens, width), BF16),
            pltpu.VMEM((nz, blk, width), BF16),
            pltpu.VMEM((nz, blk, width), BF16),
            pltpu.VMEM((groups, nr, gs * cap, width), BF16),
            pltpu.VMEM((groups, nr, gs * cap, width), BF16),
            pltpu.VMEM((gs * blk, fe), BF16),
            pltpu.VMEM((groups, nr, gs * cap, width), BF16),
            pltpu.VMEM((groups, nr, gs * cap, width), BF16),
            pltpu.VMEM((nz, blk, width), BF16),
            pltpu.VMEM((nz, blk, width), BF16),
            pltpu.VMEM((2, dqk, dv), F32),
            pltpu.VMEM((2, dqk, dv), BF16),
            pltpu.VMEM((2, dqk, dv), BF16),
            pltpu.VMEM((8, 128), F32),
            pltpu.VMEM((8, 128), F32),
            pltpu.VMEM((2, dqk // 2, dv), F32),
            pltpu.VMEM((2, dqk // 2, dv), BF16),
            pltpu.VMEM((8, 128), F32),
            pltpu.VMEM((2, dqk // 2, dv), BF16),
            pltpu.VMEM((8, 128), F32),
            pltpu.VMEM((n_pairs, hr, dv), BF16),
            pltpu.VMEM((8, 128), F32),
            pltpu.VMEM((n_pairs, hr, dv), BF16),
            pltpu.VMEM((n_pairs, 8, 128), F32),
            pltpu.VMEM((n_pairs, hr, dv), BF16),
            pltpu.VMEM((8, 128), F32),
            pltpu.VMEM((8, 128), F32),
            pltpu.VMEM((n_pairs, hr, dv), BF16),
            pltpu.VMEM((2, 2, n_pairs, hr, dv), BF16),
            pltpu.VMEM((span, dv), BF16),
            pltpu.VMEM((nx, span // nx, width), BF16),
            pltpu.VMEM((nx, span // nx, width), BF16),
            pltpu.VMEM((tokens, width), F32),
            pltpu.SemaphoreType.REGULAR,
            dma((1 + width // min(512, width),)),
            dma((16,)),
            dma((5,)),
            dma((5,)),
            dma((4,)),
            dma((4,)),
            dma((nz,)),
            dma((nz,)),
            dma((groups, nr)),
            dma((groups, nr)),
            dma((nz,)),
            dma((nz,)),
            dma((nz,)),
            dma((nz,)),
            dma((nz,)),
            dma((nz,)),
            dma((nx,)),
            dma((nx,)),
            dma((groups, nr)),
            dma((groups, nr)),
            dma((nz,)),
            dma((nz,)),
        ],
        compiler_params=pltpu.CompilerParams(
            collective_id=0, has_side_effects=True, vmem_limit_bytes=60 * 2**20
        ),
        name="layer_step",
    )(
        log_input_gate,
        forget_gate_logits,
        extra_log_forget,
        head_norm_gain.reshape(1, dv),
        expert_norm_gain.reshape(1, width),
        routes.T,
        routed_expert_weight.T,
        expert_input_tokens,
        head_key_rows,
        head_value_rows,
        queries,
        output_gate_logits,
        memory_output_matrix,
        expert_gate_matrix,
        expert_up_matrix,
        expert_down_matrix,
    )
    return pl.pallas_call(
        hand_over,
        out_shape=(
            jax.ShapeDtypeStruct(mixer_out.shape, BF16),
            jax.ShapeDtypeStruct(expert_out.shape, BF16),
        ),
        in_specs=[hbm] * 2,
        out_specs=(hbm,) * 2,
        scratch_shapes=[
            pltpu.VMEM(mixer_out.shape, BF16),
            pltpu.VMEM(expert_out.shape, BF16),
            dma((4,)),
            dma((4,)),
        ],
        compiler_params=pltpu.CompilerParams(vmem_limit_bytes=60 * 2**20),
        name="hand_over",
    )(mixer_out, expert_out)


def solution(mesh):
    nz = mesh.shape["ep"] // cores
    return jax.shard_map(
        functools.partial(body, nz, mesh.shape["tp"]),
        mesh=mesh,
        in_specs=(
            P(GRP_EP, "tp"),
            P(GRP_EP, "tp"),
            P(GRP_EP, "tp"),
            P(GRP_EP, "tp"),
            P("tp", GRP_EP),
            P("tp", GRP_EP),
            P("tp", GRP_EP),
            P("tp"),
            P("tp", None),
            P(GRP_EP_TP, None),
            P(),
            P(GRP_EP_TP, None),
            P(GRP_EP_TP, None),
            P(EP_TP, None, None),
            P(EP_TP, None, None),
            P(EP_TP, None, None),
        ),
        out_specs=(P(GRP_EP_TP, None), P(GRP_EP_TP, None)),
        check_vma=False,
    )
```
